32 devices in a mesh: rep: 2 (over x), fs: 8 (over z, y), tp: 2 (over core).
Axes of the slice: x: 2, y: 2, z: 4, core: 2. Of those that a mesh axis runs over, the one named last changes fastest.
Arguments:
- tokens: bfloat16 [12288, 2048], P(('rep', 'fs', 'tp')), may hold values from -6 to 6
- norm_gain: float32 [2048], replicated, may hold values from 0.1 to 1.9
- gate_weight: float32 [2048, 5632], P('fs', 'tp'), may hold values from -0.125 to 0.125
- up_weight: float32 [2048, 5632], P('fs', 'tp'), may hold values from -0.125 to 0.125
- gate_scale: float32 [5632], P('tp'), may hold values from 0.3 to 3
- up_scale: float32 [5632], P('tp'), may hold values from 0.3 to 3
- down_weight: float32 [5632, 2048], P('tp', 'fs'), may hold values from -0.078125 to 0.078125
- down_scale: float32 [2048], replicated, may hold values from 0.3 to 3
Outputs:
- mixed: bfloat16 [12288, 2048], P(('rep', 'fs', 'tp'))
The draws below stay inside these ranges and needn't reach their ends.
All inputs are finite; a program needn't handle non-finite values.
Results may differ from the reference program's by a relative error of at most 0.014.
Values may be sent and summed in bfloat16 or wider, within the bound.
A program may use at most 128 MiB of HBM per device.

```python
import math
import jax
import jax.numpy as jnp
from jax import lax

D = 2048
FF = 5632
TOKENS = 12288
N_TP = 2


def level_of(own_key, dims, pieces, smallest, largest):
    def one(axis_at, blocks):
        steps = jax.random.uniform(jax.random.fold_in(jax.random.fold_in(own_key, 6), axis_at), (blocks,), jnp.float32, smallest / len(pieces), largest / len(pieces))
        return jnp.repeat(jnp.exp(steps), dims[axis_at] // blocks).reshape((-1,) + (1,) * (len(dims) - axis_at - 1))

    level = one(*pieces[0])
    for cut in pieces[1:]:
        level = level * one(*cut)
    return level


def gaussian(key, extent, scale, bound, cuts=(), held_as=jnp.bfloat16):
    drawn = scale * jax.random.normal(key, extent, jnp.float32)
    if cuts:
        drawn = drawn * level_of(key, extent, cuts, -0.22, 0.18)
    return jnp.clip(drawn, -bound, bound).astype(held_as)


def setup_inputs(seed: int = 0) -> dict:
    splits = jax.random.split(jax.random.key(seed), 9)
    tokens = gaussian(splits[0], (TOKENS, D), 1.0, 6.0, ((0, 32),))
    norm_gain = jnp.clip(1.0 + 0.18 * jax.random.normal(splits[1], (D,), jnp.float32), 0.1, 1.9)
    gate_weight = gaussian(splits[2], (D, FF), D ** -0.5, 0.125, ((0, 8), (1, 2)), jnp.float32)
    up_weight = gaussian(splits[3], (D, FF), D ** -0.5, 0.125, ((0, 8), (1, 2)), jnp.float32)
    gate_scale = jnp.clip(jnp.exp(math.log(3.0) - 2.3025851 * jax.random.uniform(splits[4], (FF,), jnp.float32) ** level_of(splits[4], (FF,), ((0, 2),), -0.2, 0.2)), 0.3, 3.0)
    up_scale = jnp.clip(jnp.exp(math.log(3.0) - 2.3025851 * jax.random.uniform(splits[5], (FF,), jnp.float32) ** level_of(splits[5], (FF,), ((0, 2),), -0.2, 0.2)), 0.3, 3.0)
    down_weight = gaussian(splits[6], (FF, D), FF ** -0.5, 0.078125, ((0, 2), (1, 8)), jnp.float32)
    down_scale = jnp.clip(jnp.exp(jax.random.uniform(splits[7], (D,), jnp.float32, math.log(0.3), math.log(3.0))), 0.3, 3.0)
    return {"tokens": tokens, "norm_gain": norm_gain, "gate_weight": gate_weight, "up_weight": up_weight, "gate_scale": gate_scale, "up_scale": up_scale, "down_weight": down_weight, "down_scale": down_scale}


def reference(tokens, norm_gain, gate_weight, up_weight, gate_scale, up_scale, down_weight, down_scale):
    values = tokens.astype(jnp.float32)
    normed = (values * lax.rsqrt(lax.optimization_barrier(jnp.mean(values * values, axis=-1, keepdims=True)) + 1e-06) * norm_gain).astype(jnp.bfloat16)
    block_width = FF // N_TP
    gate_blocks = gate_weight.astype(jnp.bfloat16).reshape(D, N_TP, block_width).transpose(1, 0, 2)
    up_blocks = up_weight.astype(jnp.bfloat16).reshape(D, N_TP, block_width).transpose(1, 0, 2)
    down_blocks = down_weight.astype(jnp.bfloat16).reshape(N_TP, block_width, D)
    gate_scales = gate_scale.reshape(N_TP, block_width)
    up_scales = up_scale.reshape(N_TP, block_width)

    def one_block(running, blocks):
        gate_piece, up_piece, gate_factor, up_factor, down_piece = blocks
        gate_value = jnp.dot(normed, gate_piece, preferred_element_type=jnp.float32) * gate_factor
        up_value = jnp.dot(normed, up_piece, preferred_element_type=jnp.float32) * up_factor
        hidden = (jax.nn.silu(gate_value) * up_value).astype(jnp.bfloat16)
        partial_value = jnp.dot(hidden, down_piece, preferred_element_type=jnp.float32).astype(jnp.bfloat16)
        return (running + partial_value.astype(jnp.float32), None)
    summed, unused = lax.scan(one_block, jnp.zeros((tokens.shape[0], D), jnp.float32), (gate_blocks, up_blocks, gate_scales, up_scales, down_blocks))
    return (summed * down_scale).astype(jnp.bfloat16)
```

```python
import functools
import math

import jax
import jax.numpy as jnp
from jax import lax
from jax.experimental import pallas as pl
from jax.experimental.pallas import tpu as pltpu
from jax.sharding import PartitionSpec as P


def grid_of(count):
    inner = 1
    while (inner * 2) ** 2 <= count and count % (inner * 2) == 0:
        inner *= 2
    return count // inner, inner


def swap(x, axis):
    return lax.ppermute(x, axis, [(0, 1), (1, 0)])


def gather_kernel(outer, inner, *refs):
    local, whole = refs[:3], refs[3:6]
    own_sem, near_sem, relay_sem, cross_sem, recv_sem = refs[6:]
    me = lax.axis_index("fs")
    z, y = me // inner, lax.rem(me, inner)
    offsets = [o for o in (1, -1, 2, -2) if abs(o) < outer]

    def inside(o):
        return (z + o >= 0) & (z + o < outer)

    def peer(i):
        return z * inner + lax.rem(y + i, inner)

    barrier = pltpu.get_barrier_semaphore()
    for o in offsets:

        @pl.when(inside(o))
        def _():
            pl.semaphore_signal(
                barrier, inc=1, device_id={"fs": me + o * inner},
                device_id_type=pl.DeviceIdType.MESH,
            )

    for i in range(1, inner):
        pl.semaphore_signal(
            barrier, inc=1, device_id={"fs": peer(i)}, device_id_type=pl.DeviceIdType.MESH
        )
    reach = min(2, outer - 1)
    peers = jnp.minimum(z, reach) + jnp.minimum(outer - 1 - z, reach) + inner - 1
    pl.semaphore_wait(barrier, peers)

    def slot(a, row, column):
        return row * inner + column if a < 2 else row

    def send(a, source, row, column, target, sem):
        place = slot(a, row, column)
        return pltpu.make_async_remote_copy(
            src_ref=source,
            dst_ref=whole[a].at[place],
            send_sem=sem,
            recv_sem=recv_sem.at[a, place],
            device_id={"fs": target},
            device_id_type=pl.DeviceIdType.MESH,
        )

    def near(a, o):
        return send(a, local[a], z, y, me + o * inner, near_sem.at[a, offsets.index(o)])

    def relay(a, d):
        step = 1 if d > 0 else -1
        source = whole[a].at[slot(a, z - d, y)]
        return send(a, source, z - d, y, me + step * inner, relay_sem.at[a, outer + d])

    def cross(a, d, i):
        source = local[a] if d == 0 else whole[a].at[slot(a, z - d, y)]
        return send(a, source, z - d, y, peer(i), cross_sem.at[a, outer + d, i])

    def arrived(a, row, column):
        place = slot(a, row, column)
        return pltpu.make_async_copy(local[a], whole[a].at[place], recv_sem.at[a, place])

    def keep(a):
        return pltpu.make_async_copy(local[a], whole[a].at[slot(a, z, y)], own_sem.at[a])

    def take(a, d):
        @pl.when(inside(-d))
        def _():
            arrived(a, z - d, y).wait()
            if a < 2:
                for i in range(1, inner):
                    cross(a, d, i).start()
            if abs(d) >= 2:
                step = 1 if d > 0 else -1

                @pl.when(inside(step))
                def _():
                    relay(a, d).start()

    def open_near(a, o):
        @pl.when(inside(o))
        def _():
            near(a, o).start()

    distances = [d * sign for d in range(1, outer) for sign in (1, -1)]
    for o in offsets[:2]:
        open_near(0, o)
    for i in range(1, inner):
        cross(0, 0, i).start()
    for o in offsets[:2]:
        open_near(1, o)
    for i in range(1, inner):
        cross(1, 0, i).start()
    for a in range(2):
        for o in offsets[2:]:
            open_near(a, o)
    for a in range(3):
        keep(a).start()
    for d in distances[:4]:
        for a in range(2):
            take(a, d)
    for o in offsets:
        open_near(2, o)
    for d in distances[4:]:
        for a in range(2):
            take(a, d)
    for d in distances:
        take(2, d)

    for a in range(3):
        keep(a).wait()
        for o in offsets:

            @pl.when(inside(o))
            def _():
                near(a, o).wait_send()

        for d in distances:
            if abs(d) >= 2:

                @pl.when(inside(-d) & inside(1 if d > 0 else -1))
                def _():
                    relay(a, d).wait_send()

    for a in range(2):
        for d in [0] + distances:

            @pl.when(inside(-d))
            def _():
                for i in range(1, inner):
                    cross(a, d, i).wait_send()
                    arrived(a, z - d, lax.rem(y + i, inner)).wait()


def gather_weights(outer, inner, gate, up, down):
    shapes = [(outer * inner, *gate.shape), (outer * inner, *up.shape), (outer, *down.shape)]
    anywhere = pl.BlockSpec(memory_space=pl.ANY)
    return pl.pallas_call(
        functools.partial(gather_kernel, outer, inner),
        out_shape=[jax.ShapeDtypeStruct(shape, gate.dtype) for shape in shapes],
        in_specs=[anywhere] * 3,
        out_specs=[anywhere] * 3,
        scratch_shapes=[
            pltpu.SemaphoreType.DMA((3,)),
            pltpu.SemaphoreType.DMA((3, 4)),
            pltpu.SemaphoreType.DMA((3, 2 * outer)),
            pltpu.SemaphoreType.DMA((2, 2 * outer, inner)),
            pltpu.SemaphoreType.DMA((3, outer * inner)),
        ],
        compiler_params=pltpu.CompilerParams(collective_id=0, has_side_effects=True),
        cost_estimate=pl.CostEstimate(
            flops=0, bytes_accessed=32 * sum(math.prod(shape) for shape in shapes), transcendentals=0
        ),
    )(gate, up, down)


def roll(x, shift):
    return lax.dynamic_slice_in_dim(jnp.concatenate([x, x], -1), shift, x.shape[-1], x.ndim - 1)


def reorder(x, outer, inner, y):
    block = x.shape[-1] // (outer * inner)
    position = lax.broadcasted_iota(jnp.int32, x.shape, x.ndim - 1) % (inner * block)
    ahead = roll(x, y * block)
    behind = roll(x, (x.shape[-1] - inner * block + y * block) % x.shape[-1])
    return jnp.where(position + y * block < inner * block, ahead, behind)


def gather_rows(x, axis):
    if lax.axis_size(axis) == 2:
        return jnp.stack([x, swap(x, axis)])
    return lax.all_gather(x, axis)


def reduce_rows(x, axis):
    if lax.axis_size(axis) == 2:
        return x[0].astype(jnp.float32) + swap(x[1].astype(jnp.bfloat16), axis).astype(jnp.float32)
    return lax.psum_scatter(
        x.astype(jnp.bfloat16), axis, scatter_dimension=0, tiled=False
    ).astype(jnp.float32)


def on_device(
    tokens, norm_gain, gate_weight, up_weight, gate_scale, up_scale, down_weight, down_scale
):
    groups, count = lax.axis_size("rep"), lax.axis_size("fs")
    tps = lax.axis_size("tp")
    outer, inner = grid_of(count)
    y = lax.axis_index("fs") % inner
    width = gate_weight.shape[1] // groups
    start = lax.axis_index("rep") * width
    gate_local, up_local = (
        lax.dynamic_slice_in_dim(weight, start, width, 1).astype(jnp.bfloat16)
        for weight in (gate_weight, up_weight)
    )
    down_local = lax.dynamic_slice_in_dim(down_weight, start, width, 0).astype(jnp.bfloat16)
    gate_scale, up_scale = (
        lax.dynamic_slice_in_dim(scale, start, width, 0) for scale in (gate_scale, up_scale)
    )

    gate_whole, up_whole, down_near = gather_weights(
        outer, inner, gate_local, up_local, down_local
    )

    values = tokens.astype(jnp.float32)
    own_normed = (
        values * lax.rsqrt(jnp.mean(values * values, axis=-1, keepdims=True) + 1e-06) * norm_gain
    ).astype(jnp.bfloat16)
    rows, depth = own_normed.shape
    normed = gather_rows(gather_rows(own_normed, "tp"), "rep").swapaxes(0, 1).reshape(-1, depth)

    gate_whole, up_whole = gate_whole.reshape(depth, width), up_whole.reshape(depth, width)
    cuts = [slice(0, outer // 2), slice(outer // 2, outer)] if outer > 1 else [slice(0, 1)]
    pieces = [down_near[cut] for cut in cuts]
    for i in range(1, inner):
        pairs = [(f, f - f % inner + (f - i) % inner) for f in range(count)]
        pieces += [lax.ppermute(down_near[cut], "fs", pairs) for cut in cuts]
    gate_value = jnp.dot(normed, gate_whole, preferred_element_type=jnp.float32)
    up_value = jnp.dot(normed, up_whole, preferred_element_type=jnp.float32)
    hidden = (jax.nn.silu(gate_value * gate_scale) * (up_value * up_scale)).astype(jnp.bfloat16)

    near = len(cuts)
    later, pieces[near:] = lax.optimization_barrier((hidden, pieces[near:]))
    block = down_local.shape[1]
    columns = []
    for at, piece in enumerate(pieces):
        partial_value = jnp.dot(
            hidden if at < near else later, jnp.concatenate(list(piece), 1), preferred_element_type=jnp.float32
        ).astype(jnp.bfloat16)
        partial_value = partial_value.reshape(tps, groups, rows, -1)
        total = reduce_rows(reduce_rows(partial_value, "tp"), "rep")
        columns += [total[:, c * block : (c + 1) * block] for c in range(len(piece))]
    summed = jnp.concatenate([columns[i * outer + a] for a in range(outer) for i in range(inner)], -1)
    scale = reorder(down_scale[None], outer, inner, y)
    mixed = (summed * scale).astype(jnp.bfloat16)
    return reorder(mixed, outer, inner, (inner - y) % inner)


def hidden_chunks(width):
    step = 256
    return [(at, min(at + step, width)) for at in range(0, width, step)]


def paired(gate, up):
    out = []
    for lo, hi in hidden_chunks(gate.shape[-1]):
        whole = lo + (hi - lo) // 128 * 128
        parts = [gate[..., lo:whole], up[..., lo:whole]]
        if whole < hi:
            parts += [gate[..., whole:hi], up[..., whole:hi]]
        out.append(jnp.concatenate(parts, -1))
    return out


def layer_kernel(outer, chunks, split, *refs):
    n = len(chunks)
    tok, gus, down, scale, down_scale, out = refs[0], refs[1 : n + 1], *refs[n + 1 : n + 5]
    refs = refs[n + 5 :]
    allx, held, hid, part = refs[0], refs[1 : n + 2], *refs[n + 2 : n + 4]
    refs = refs[n + 4 :]
    got_a, sum_a, sum_b, got_ba, got_bb, keep_a, keep_b, next_a, next_b, got_ca, got_cb = refs[:11]
    (
        w_own, w_recv, w_y, w_z, t_own, t_recv, t_send,
        a_send, a_recv, b_send, b_recv, c_send, c_recv,
    ) = refs[11:]
    items = n + 1
    sources = [*gus, down]
    x, me, c = lax.axis_index("rep"), lax.axis_index("fs"), lax.axis_index("tp")
    z, y = me // 2, lax.rem(me, 2)
    rows, block = tok.shape[0], down.shape[2]
    height = down.shape[1]
    half = block // 2
    to_core, to_x, to_y = {"tp": 1 - c}, {"rep": 1 - x}, {"fs": z * 2 + 1 - y}
    up_ok, down_ok = z + 1 < outer, z > 0

    def at_z(step):
        return {"fs": me + 2 * step}

    barrier = pltpu.get_barrier_semaphore()

    def greet(target):
        pl.semaphore_signal(
            barrier, inc=1, device_id=target, device_id_type=pl.DeviceIdType.MESH
        )

    for target in (to_core, to_x, to_y):
        greet(target)

    @pl.when(down_ok)
    def _():
        greet(at_z(-1))

    @pl.when(up_ok)
    def _():
        greet(at_z(1))

    pl.semaphore_wait(
        barrier, 3 + jnp.minimum(z, 1) + jnp.minimum(outer - 1 - z, 1)
    )

    def remote(source, target, send_sem, recv_sem, device):
        return pltpu.make_async_remote_copy(
            src_ref=source, dst_ref=target, send_sem=send_sem, recv_sem=recv_sem,
            device_id=device, device_id_type=pl.DeviceIdType.MESH,
        )

    def done(ref, sem):
        pltpu.make_async_copy(ref, ref, sem).wait()


    def slot(i, f):
        return held[i].at[f] if i < n else held[i].at[f, pl.ds(0, height)]

    def own_copy(i):
        return pltpu.make_async_copy(sources[i].at[y], slot(i, me), w_own.at[i])

    def across_y(i):
        return remote(sources[i].at[1 - y], slot(i, me), w_y.at[i], w_recv.at[i, me], to_y)

    def along(i, f, source, step):
        side = 0 if step < 0 else 1
        return remote(source, slot(i, f), w_z.at[i, f, side], w_recv.at[i, f], at_z(step))

    def send_z(i, f, source, step):
        @pl.when(down_ok if step < 0 else up_ok)
        def _():
            along(i, f, source, step).start()

    other = z * 2 + 1 - y

    def send_own(i, steps=(-1, 1)):
        for step in steps:
            send_z(i, me, sources[i].at[y], step)

    def take_other(i):
        done(slot(i, other), w_recv.at[i, other])

    def send_other(i, steps=(-1, 1)):
        for step in steps:
            send_z(i, other, slot(i, other), step)

    def take(i, d, qs=(0, 1)):
        for sign in (1, -1):
            s = z + sign * d

            @pl.when((s < outer) if sign > 0 else (s >= 0))
            def _():
                for q in qs:
                    f = s * 2 + q
                    done(slot(i, f), w_recv.at[i, f])
                    send_z(i, f, slot(i, f), -sign)


    def place(cc, xx, yy):
        return cc * 4 + xx * 2 + yy

    spans = (pl.ds(0, split), pl.ds(split, rows - split))

    def move(t, h, source, device, at):
        return remote(
            source, allx.at[t, spans[h]], t_send.at[at], t_recv.at[t, h], device
        )

    mine, near_x, near_y, diagonal = (
        place(c, x, y), place(c, 1 - x, y), place(c, x, 1 - y), place(c, 1 - x, 1 - y)
    )

    def moved(t, h):
        done(allx.at[t, spans[h]], t_recv.at[t, h])

    own_tokens = pltpu.make_async_copy(tok, allx.at[mine], t_own.at[0])
    own_sends = [
        [move(mine, h, tok.at[spans[h]], to_x, 2 * h) for h in range(2)],
        [move(mine, h, tok.at[spans[h]], to_y, 2 * h + 1) for h in range(2)],
    ]
    relay_y = move(near_x, 0, allx.at[near_x, spans[0]], to_y, 4)
    relay_x = move(near_y, 1, allx.at[near_y, spans[1]], to_x, 5)

    def share(t, source, at):
        return remote(source, allx.at[t], t_send.at[at], t_recv.at[t, 0], to_core)

    shares = [
        share(mine, tok, 6),
        share(near_x, allx.at[near_x], 7),
        share(near_y, allx.at[near_y], 8),
        share(diagonal, allx.at[diagonal], 9),
    ]

    across_y(0).start()
    send_own(0)
    for h in range(2):
        own_sends[0][h].start()
    own_sends[1][1].start()
    across_y(1).start()
    own_sends[1][0].start()
    for i in range(2, items):
        across_y(i).start()
    shares[0].start()
    own_tokens.start()
    for i in range(items):
        own_copy(i).start()

    tail = held[n].shape[1] - height
    if tail:
        for f in range(2 * outer):
            held[n][f, height:, :] = jnp.zeros((tail, block), held[n].dtype)

    take_other(0)
    send_other(0)
    send_own(1)
    moved(near_x, 0)
    relay_y.start()
    take(0, 1)
    moved(near_y, 1)
    relay_x.start()
    take_other(1)
    send_other(1)
    for d in range(2, outer):
        take(0, d)
    send_own(2)
    moved(near_x, 1)
    shares[1].start()
    moved(near_y, 0)
    shares[2].start()
    take(1, 1)
    take_other(2)
    send_other(2)
    for d in range(2, outer - 1):
        take(1, d)
    moved(diagonal, 0)
    moved(diagonal, 1)
    shares[3].start()
    own_tokens.wait()
    for xx in range(2):
        for yy in range(2):
            t = place(1 - c, xx, yy)
            done(allx.at[t], t_recv.at[t, 0])


    starts = [0]
    for lo, hi in chunks:
        starts.append(starts[-1] + 2 * (hi - lo))
    depth = tok.shape[1]

    def silu(v):
        return v * (1.0 / (1.0 + jnp.exp(-v)))

    def hidden(i):
        lo, hi = chunks[i]
        even = (hi - lo) // 128 * 128
        odd = hi - lo - even
        own_copy(i).wait()

        def body(t, carry):
            both = jnp.dot(
                allx[t], held[i][...].reshape(depth, 2 * (hi - lo)),
                preferred_element_type=jnp.float32,
            ) * scale[:, starts[i] : starts[i + 1]]
            if even:
                value = silu(both[:, :even]) * both[:, even : 2 * even]
                hid[t, :, lo : lo + even] = value.astype(hid.dtype)
            if odd:
                last = both[:, 2 * even :]
                value = silu(last) * pltpu.roll(last, odd, 1)
                lane = lax.broadcasted_iota(jnp.int32, value.shape, 1)
                hid[t, :, lo + even : lo + even + 2 * odd] = jnp.where(
                    lane < odd, value, 0.0
                ).astype(hid.dtype)
            return carry

        lax.fori_loop(0, 8, body, 0)

    def open_down(d):
        @pl.when(z == outer - 1 - d)
        def _():
            send_own(n, (-1,))
            send_other(n, (-1,))

        @pl.when(z == d)
        def _():
            send_own(n, (1,))
            send_other(n, (1,))

    hidden(0)
    for d in range(max(outer - 1, 2), outer):
        take(1, d)
    take(2, 1)
    hidden(1)
    take_other(n)
    open_down(0)
    open_down(1)
    for d in range(2, outer):
        take(2, d)
        open_down(d)
    for i in range(2, n):
        hidden(i)


    planes = []
    for spot in range(outer):
        plane = 0
        for zz in range(outer):
            order = sorted(range(outer), key=lambda s: (abs(s - zz), -s))
            plane = plane + jnp.where(z == zz, order[spot], 0)
        planes.append(plane)
    blocks = [planes[k // 2] * 2 + k % 2 for k in range(2 * outer)]

    def send_a(k):
        return remote(
            part.at[k % 3, pl.ds((1 - c) * 4, 4)], got_a.at[k], a_send.at[k], a_recv.at[k], to_core
        )

    def send_b(k):
        return [
            remote(
                sum_a.at[k % 3, pl.ds((1 - x) * 2, 2)], got_ba.at[k],
                b_send.at[k, 0], b_recv.at[k, 0], to_x,
            ),
            remote(
                sum_b.at[k % 3, pl.ds((1 - y) * 2, 2)], got_bb.at[k],
                b_send.at[k, 1], b_recv.at[k, 1], to_y,
            ),
        ]

    def send_c(k):
        return [
            remote(next_a.at[k % 3], got_ca.at[k], c_send.at[k, 0], c_recv.at[k, 0], to_y),
            remote(next_b.at[k % 3], got_cb.at[k], c_send.at[k, 1], c_recv.at[k, 1], to_x),
        ]

    def multiply(k):
        if k >= 3:
            send_a(k - 3).wait_send()
        f = blocks[k]

        def body(t, carry):
            part[k % 3, t] = jnp.dot(
                hid[t], held[n][f], preferred_element_type=jnp.float32
            ).astype(part.dtype)
            return carry

        lax.fori_loop(0, 8, body, 0)
        send_a(k).start()

    def wide(value):
        return value.astype(jnp.float32)

    def first(k):
        done(got_a.at[k], a_recv.at[k])
        if k >= 3:
            for copy in send_b(k - 3):
                copy.wait_send()

        def body(i, carry):
            total = (wide(part[k % 3, c * 4 + i]) + wide(got_a[k, i])).astype(part.dtype)
            sum_a[k % 3, i] = total[:, :half]
            sum_b[k % 3, lax.rem(i, 2) * 2 + i // 2] = total[:, half:]
            return carry

        lax.fori_loop(0, 4, body, 0)
        for copy in send_b(k):
            copy.start()

    def second(k):
        done(got_ba.at[k], b_recv.at[k, 0])
        done(got_bb.at[k], b_recv.at[k, 1])
        if k >= 3:
            for copy in send_c(k - 3):
                copy.wait_send()
        s = k % 3
        next_a[s] = (wide(sum_a[s, x * 2 + 1 - y]) + wide(got_ba[k, 1 - y])).astype(next_a.dtype)
        next_b[s] = (wide(sum_b[s, y * 2 + 1 - x]) + wide(got_bb[k, 1 - x])).astype(next_b.dtype)
        for copy in send_c(k):
            copy.start()
        keep_a[s] = wide(sum_a[s, x * 2 + y]) + wide(got_ba[k, y])
        keep_b[s] = wide(sum_b[s, y * 2 + x]) + wide(got_bb[k, x])

    def third(k):
        done(got_ca.at[k], c_recv.at[k, 0])
        done(got_cb.at[k], c_recv.at[k, 1])
        s = k % 3
        for keep, got, lead in ((keep_a, got_ca, 0), (keep_b, got_cb, half)):
            at = pl.ds(pl.multiple_of(blocks[k] * block + lead, half), half)
            out[:, at] = ((keep[s] + wide(got[k])) * down_scale[:, at]).astype(out.dtype)

    def finish():
        for i in range(items):
            across_y(i).wait_send()
            for step in (-1, 1):
                for d in range(outer):
                    s = z - step * d

                    @pl.when(((s < outer) & down_ok) if step < 0 else ((s >= 0) & up_ok))
                    def _():
                        for q in range(2):
                            f = s * 2 + q
                            along(i, f, slot(i, f), step).wait_send()

        for copy in (*own_sends[0], *own_sends[1], relay_y, relay_x, *shares):
            copy.wait_send()
        for k in range(max(2 * outer - 3, 0), 2 * outer):
            for copy in (send_a(k), *send_b(k), *send_c(k)):
                copy.wait_send()

    inside = down_ok & up_ok
    early = {1: (1, 0), 2: (1, 1), 3: (2, 0), 4: (2, 1)} if outer == 4 else {}
    own_copy(n).wait()
    for k in range(2 * outer + 3):
        if 0 <= k - 1 < 2 * outer:
            first(k - 1)
        if 0 <= k - 2 < 2 * outer:
            second(k - 2)
        if 0 <= k - 3 < 2 * outer:
            third(k - 3)
        if k < 2 * outer:
            if k in early:

                @pl.when(inside)
                def _():
                    take(n, early[k][0], early[k][1:])

            if k >= 2:

                @pl.when(jnp.logical_not(inside))
                def _():
                    take(n, k // 2, (k % 2,))

            multiply(k)
    finish()


def fused_layer(outer, chunks, tok, gus, down, scale, down_scale):
    rows, depth = tok.shape
    count, height, block = 2 * outer, down.shape[1], down.shape[2]
    padded = -(-height // 128) * 128
    n = len(chunks)
    kind = tok.dtype

    def room(*shape, dtype=kind):
        return pltpu.VMEM(shape, dtype)

    anywhere = pl.BlockSpec(memory_space=pl.ANY)
    inside = pl.BlockSpec(memory_space=pltpu.VMEM)
    dma = pltpu.SemaphoreType.DMA
    split = rows // 96 * 16
    return pl.pallas_call(
        functools.partial(layer_kernel, outer, chunks, split),
        out_shape=jax.ShapeDtypeStruct((rows, depth), kind),
        in_specs=[anywhere] * (n + 2) + [inside] * 2,
        out_specs=inside,
        scratch_shapes=[
            room(8, rows, depth),
            *(room(count, *gu.shape[1:]) for gu in gus),
            room(count, padded, block),
            room(8, rows, padded),
            room(3, 8, rows, block),
            room(count, 4, rows, block),
            room(3, 4, rows, block // 2),
            room(3, 4, rows, block // 2),
            room(count, 2, rows, block // 2),
            room(count, 2, rows, block // 2),
            room(3, rows, block // 2, dtype=jnp.float32),
            room(3, rows, block // 2, dtype=jnp.float32),
            room(3, rows, block // 2),
            room(3, rows, block // 2),
            room(count, rows, block // 2),
            room(count, rows, block // 2),
            dma((n + 1,)),
            dma((n + 1, count)),
            dma((n + 1,)),
            dma((n + 1, count, 2)),
            dma((1,)),
            dma((8, 2)),
            dma((10,)),
            dma((count,)),
            dma((count,)),
            dma((count, 2)),
            dma((count, 2)),
            dma((count, 2)),
            dma((count, 2)),
        ],
        compiler_params=pltpu.CompilerParams(
            collective_id=1, has_side_effects=True, vmem_limit_bytes=60 * 1024 * 1024
        ),
        cost_estimate=pl.CostEstimate(
            flops=48 * rows * depth * height, bytes_accessed=8 * rows * depth, transcendentals=0
        ),
    )(tok, *gus, down, scale, down_scale)


def on_plane(
    tokens, norm_gain, gate_weight, up_weight, gate_scale, up_scale, down_weight, down_scale
):
    outer, _ = grid_of(lax.axis_size("fs"))
    x, y = lax.axis_index("rep"), lax.axis_index("fs") % 2
    width = gate_weight.shape[1] // 4
    chunks = hidden_chunks(width)
    gate, up = (
        lax.dynamic_slice_in_dim(weight, x * 2 * width, 2 * width, 1).astype(jnp.bfloat16)
        for weight in (gate_weight, up_weight)
    )
    pieces = [paired(gate[:, s], up[:, s]) for s in (slice(0, width), slice(width, 2 * width))]
    gus = [jnp.stack(pair) for pair in zip(*pieces)]
    down = lax.dynamic_slice_in_dim(down_weight, x * 2 * width, 2 * width, 0).astype(jnp.bfloat16)
    down = down.reshape(2, width, -1)
    scales = [
        lax.dynamic_slice_in_dim(scale[None], (x * 2 + y) * width, width, 1)
        for scale in (gate_scale, up_scale)
    ]
    scale = jnp.concatenate(paired(*scales), 1)
    values = tokens.astype(jnp.float32)
    normed = (
        values * lax.rsqrt(jnp.mean(values * values, axis=-1, keepdims=True) + 1e-06) * norm_gain
    ).astype(jnp.bfloat16)
    return fused_layer(outer, chunks, normed, gus, down, scale, down_scale[None])


def planar(mesh, tokens, gate_weight):
    sizes = mesh.shape
    if grid_of(sizes["fs"]) != (4, 2) or sizes["rep"] != 2 or sizes["tp"] != 2:
        return False
    width, rows = gate_weight.shape[1] // 8, tokens.shape[0] // mesh.size
    depth = gate_weight.shape[0]
    return (
        gate_weight.shape[1] % 8 == 0 and width % 128 in (0, 64) and width > 512
        and rows % 96 == 0 and depth % (sizes["fs"] * 256) == 0
    )


def solution(mesh):
    placed = (
        P(("rep", "fs", "tp"), None),
        P(),
        P("fs", "tp"),
        P("fs", "tp"),
        P("tp"),
        P("tp"),
        P("tp", "fs"),
        P(),
    )

    def layer(tokens, norm_gain, gate_weight, *rest):
        return jax.shard_map(
            on_plane if planar(mesh, tokens, gate_weight) else on_device,
            mesh=mesh,
            in_specs=placed,
            out_specs=P(("rep", "fs", "tp"), None),
            check_vma=False,
        )(tokens, norm_gain, gate_weight, *rest)

    return layer
```

```python
import functools
import math

import jax
import jax.numpy as jnp
from jax import lax
from jax.experimental import pallas as pl
from jax.experimental.pallas import tpu as pltpu
from jax.sharding import PartitionSpec as P


def grid_of(count):
    inner = 1
    while (inner * 2) ** 2 <= count and count % (inner * 2) == 0:
        inner *= 2
    return count // inner, inner


def swap(x, axis):
    return lax.ppermute(x, axis, [(0, 1), (1, 0)])


def gather_kernel(outer, inner, *refs):
    local, whole = refs[:3], refs[3:6]
    own_sem, near_sem, relay_sem, cross_sem, recv_sem = refs[6:]
    me = lax.axis_index("fs")
    z, y = me // inner, lax.rem(me, inner)
    offsets = [o for o in (1, -1, 2, -2) if abs(o) < outer]

    def inside(o):
        return (z + o >= 0) & (z + o < outer)

    def peer(i):
        return z * inner + lax.rem(y + i, inner)

    barrier = pltpu.get_barrier_semaphore()
    for o in offsets:

        @pl.when(inside(o))
        def _():
            pl.semaphore_signal(
                barrier, inc=1, device_id={"fs": me + o * inner},
                device_id_type=pl.DeviceIdType.MESH,
            )

    for i in range(1, inner):
        pl.semaphore_signal(
            barrier, inc=1, device_id={"fs": peer(i)}, device_id_type=pl.DeviceIdType.MESH
        )
    reach = min(2, outer - 1)
    peers = jnp.minimum(z, reach) + jnp.minimum(outer - 1 - z, reach) + inner - 1
    pl.semaphore_wait(barrier, peers)

    def slot(a, row, column):
        return row * inner + column if a < 2 else row

    def send(a, source, row, column, target, sem):
        place = slot(a, row, column)
        return pltpu.make_async_remote_copy(
            src_ref=source,
            dst_ref=whole[a].at[place],
            send_sem=sem,
            recv_sem=recv_sem.at[a, place],
            device_id={"fs": target},
            device_id_type=pl.DeviceIdType.MESH,
        )

    def near(a, o):
        return send(a, local[a], z, y, me + o * inner, near_sem.at[a, offsets.index(o)])

    def relay(a, d):
        step = 1 if d > 0 else -1
        source = whole[a].at[slot(a, z - d, y)]
        return send(a, source, z - d, y, me + step * inner, relay_sem.at[a, outer + d])

    def cross(a, d, i):
        source = local[a] if d == 0 else whole[a].at[slot(a, z - d, y)]
        return send(a, source, z - d, y, peer(i), cross_sem.at[a, outer + d, i])

    def arrived(a, row, column):
        place = slot(a, row, column)
        return pltpu.make_async_copy(local[a], whole[a].at[place], recv_sem.at[a, place])

    def keep(a):
        return pltpu.make_async_copy(local[a], whole[a].at[slot(a, z, y)], own_sem.at[a])

    def take(a, d):
        @pl.when(inside(-d))
        def _():
            arrived(a, z - d, y).wait()
            if a < 2:
                for i in range(1, inner):
                    cross(a, d, i).start()
            if abs(d) >= 2:
                step = 1 if d > 0 else -1

                @pl.when(inside(step))
                def _():
                    relay(a, d).start()

    def open_near(a, o):
        @pl.when(inside(o))
        def _():
            near(a, o).start()

    distances = [d * sign for d in range(1, outer) for sign in (1, -1)]
    for o in offsets[:2]:
        open_near(0, o)
    for i in range(1, inner):
        cross(0, 0, i).start()
    for o in offsets[:2]:
        open_near(1, o)
    for i in range(1, inner):
        cross(1, 0, i).start()
    for a in range(2):
        for o in offsets[2:]:
            open_near(a, o)
    for a in range(3):
        keep(a).start()
    for d in distances[:4]:
        for a in range(2):
            take(a, d)
    for o in offsets:
        open_near(2, o)
    for d in distances[4:]:
        for a in range(2):
            take(a, d)
    for d in distances:
        take(2, d)

    for a in range(3):
        keep(a).wait()
        for o in offsets:

            @pl.when(inside(o))
            def _():
                near(a, o).wait_send()

        for d in distances:
            if abs(d) >= 2:

                @pl.when(inside(-d) & inside(1 if d > 0 else -1))
                def _():
                    relay(a, d).wait_send()

    for a in range(2):
        for d in [0] + distances:

            @pl.when(inside(-d))
            def _():
                for i in range(1, inner):
                    cross(a, d, i).wait_send()
                    arrived(a, z - d, lax.rem(y + i, inner)).wait()


def gather_weights(outer, inner, gate, up, down):
    shapes = [(outer * inner, *gate.shape), (outer * inner, *up.shape), (outer, *down.shape)]
    anywhere = pl.BlockSpec(memory_space=pl.ANY)
    return pl.pallas_call(
        functools.partial(gather_kernel, outer, inner),
        out_shape=[jax.ShapeDtypeStruct(shape, gate.dtype) for shape in shapes],
        in_specs=[anywhere] * 3,
        out_specs=[anywhere] * 3,
        scratch_shapes=[
            pltpu.SemaphoreType.DMA((3,)),
            pltpu.SemaphoreType.DMA((3, 4)),
            pltpu.SemaphoreType.DMA((3, 2 * outer)),
            pltpu.SemaphoreType.DMA((2, 2 * outer, inner)),
            pltpu.SemaphoreType.DMA((3, outer * inner)),
        ],
        compiler_params=pltpu.CompilerParams(collective_id=0, has_side_effects=True),
        cost_estimate=pl.CostEstimate(
            flops=0, bytes_accessed=32 * sum(math.prod(shape) for shape in shapes), transcendentals=0
        ),
    )(gate, up, down)


def roll(x, shift):
    return lax.dynamic_slice_in_dim(jnp.concatenate([x, x], -1), shift, x.shape[-1], x.ndim - 1)


def reorder(x, outer, inner, y):
    block = x.shape[-1] // (outer * inner)
    position = lax.broadcasted_iota(jnp.int32, x.shape, x.ndim - 1) % (inner * block)
    ahead = roll(x, y * block)
    behind = roll(x, (x.shape[-1] - inner * block + y * block) % x.shape[-1])
    return jnp.where(position + y * block < inner * block, ahead, behind)


def gather_rows(x, axis):
    if lax.axis_size(axis) == 2:
        return jnp.stack([x, swap(x, axis)])
    return lax.all_gather(x, axis)


def reduce_rows(x, axis):
    if lax.axis_size(axis) == 2:
        return x[0].astype(jnp.float32) + swap(x[1].astype(jnp.bfloat16), axis).astype(jnp.float32)
    return lax.psum_scatter(
        x.astype(jnp.bfloat16), axis, scatter_dimension=0, tiled=False
    ).astype(jnp.float32)


def on_device(
    tokens, norm_gain, gate_weight, up_weight, gate_scale, up_scale, down_weight, down_scale
):
    groups, count = lax.axis_size("rep"), lax.axis_size("fs")
    tps = lax.axis_size("tp")
    outer, inner = grid_of(count)
    y = lax.axis_index("fs") % inner
    width = gate_weight.shape[1] // groups
    start = lax.axis_index("rep") * width
    gate_local, up_local = (
        lax.dynamic_slice_in_dim(weight, start, width, 1).astype(jnp.bfloat16)
        for weight in (gate_weight, up_weight)
    )
    down_local = lax.dynamic_slice_in_dim(down_weight, start, width, 0).astype(jnp.bfloat16)
    gate_scale, up_scale = (
        lax.dynamic_slice_in_dim(scale, start, width, 0) for scale in (gate_scale, up_scale)
    )

    gate_whole, up_whole, down_near = gather_weights(
        outer, inner, gate_local, up_local, down_local
    )

    values = tokens.astype(jnp.float32)
    own_normed = (
        values * lax.rsqrt(jnp.mean(values * values, axis=-1, keepdims=True) + 1e-06) * norm_gain
    ).astype(jnp.bfloat16)
    rows, depth = own_normed.shape
    normed = gather_rows(gather_rows(own_normed, "tp"), "rep").swapaxes(0, 1).reshape(-1, depth)

    gate_whole, up_whole = gate_whole.reshape(depth, width), up_whole.reshape(depth, width)
    cuts = [slice(0, outer // 2), slice(outer // 2, outer)] if outer > 1 else [slice(0, 1)]
    pieces = [down_near[cut] for cut in cuts]
    for i in range(1, inner):
        pairs = [(f, f - f % inner + (f - i) % inner) for f in range(count)]
        pieces += [lax.ppermute(down_near[cut], "fs", pairs) for cut in cuts]
    gate_value = jnp.dot(normed, gate_whole, preferred_element_type=jnp.float32)
    up_value = jnp.dot(normed, up_whole, preferred_element_type=jnp.float32)
    hidden = (jax.nn.silu(gate_value * gate_scale) * (up_value * up_scale)).astype(jnp.bfloat16)

    near = len(cuts)
    later, pieces[near:] = lax.optimization_barrier((hidden, pieces[near:]))
    block = down_local.shape[1]
    columns = []
    for at, piece in enumerate(pieces):
        partial_value = jnp.dot(
            hidden if at < near else later, jnp.concatenate(list(piece), 1), preferred_element_type=jnp.float32
        ).astype(jnp.bfloat16)
        partial_value = partial_value.reshape(tps, groups, rows, -1)
        total = reduce_rows(reduce_rows(partial_value, "tp"), "rep")
        columns += [total[:, c * block : (c + 1) * block] for c in range(len(piece))]
    summed = jnp.concatenate([columns[i * outer + a] for a in range(outer) for i in range(inner)], -1)
    scale = reorder(down_scale[None], outer, inner, y)
    mixed = (summed * scale).astype(jnp.bfloat16)
    return reorder(mixed, outer, inner, (inner - y) % inner)


def hidden_chunks(width):
    whole = width // 128 * 128
    return [(0, whole - 256), (whole - 256, whole - 128), (whole, width), (whole - 128, whole)]


def columns(value, at, count):
    shift = at % 128
    if shift == 0:
        return value[:, at : at + count]
    low, high = at - shift, min(at - shift + count + 128, value.shape[1])
    return pltpu.roll(value[:, low:high], high - low - shift, 1)[:, :count]


def joined(gate, up, part, lo, hi):
    at = part * (gate.shape[1] // 2) + lo
    odd = (hi - lo) % 128
    even = hi - lo - odd
    pieces = [columns(gate, at, even), columns(up, at, even)] if even else []
    if odd:
        left = columns(gate, at + even, 128)
        right = pltpu.roll(columns(up, at + even, 128), odd, 1)
        lane = lax.broadcasted_iota(jnp.int32, left.shape, 1)
        pieces.append(jnp.where(lane < odd, left, right))
    return pieces


def units_of(outer, block):
    units = [(k // 2, k % 2, 0, block) for k in range(2 * outer - 1)]
    half = block // 2
    return units + [(outer - 1, 1, 0, half), (outer - 1, 1, half, half)]


def layer_kernel(outer, chunks, split, *refs):
    n = len(chunks)
    tokens, gain, gate, up, gate_scale, up_scale, down, down_scale, out = refs[:9]
    refs = refs[9:]
    raw_tok, raw_gate, raw_up, raw_down, scale = refs[:5]
    spare, allx, held, hid, part = refs[5 : n + 6], refs[n + 6], refs[n + 7 : 2 * n + 8], *refs[2 * n + 8 : 2 * n + 10]
    refs = refs[2 * n + 10 :]
    got_a, sum_a, sum_b, got_ba, got_bb, keep_a, keep_b, next_a, next_b, got_ca, got_cb, result, early_sum, head_sum = refs[:14]
    (
        raw_sem, w_recv, w_y, w_z, t_recv, t_send,
        a_send, a_recv, b_send, b_recv, c_send, c_recv,
    ) = refs[14:]
    items = n + 2
    x, me, c = lax.axis_index("rep"), lax.axis_index("fs"), lax.axis_index("tp")
    z, y = me // 2, lax.rem(me, 2)
    other = z * 2 + 1 - y
    rows, depth = raw_tok.shape
    height, block = spare[n].shape
    half = block // 2
    to_core, to_x, to_y = {"tp": 1 - c}, {"rep": 1 - x}, {"fs": other}
    up_ok, down_ok = z + 1 < outer, z > 0
    inside = down_ok & up_ok

    def at_z(step):
        return {"fs": me + 2 * step}

    span = pl.ds(pl.multiple_of(x * (2 * height), 128), 2 * height)
    loads = [
        pltpu.make_async_copy(gate.at[:, span], raw_gate, raw_sem.at[0]),
        pltpu.make_async_copy(up.at[:, span], raw_up, raw_sem.at[1]),
        pltpu.make_async_copy(tokens, raw_tok, raw_sem.at[2]),
        pltpu.make_async_copy(down.at[span], raw_down, raw_sem.at[3]),
    ]
    for load in loads:
        load.start()

    barrier = pltpu.get_barrier_semaphore()

    def greet(target):
        pl.semaphore_signal(
            barrier, inc=1, device_id=target, device_id_type=pl.DeviceIdType.MESH
        )

    for target in (to_core, to_x, to_y):
        greet(target)

    @pl.when(down_ok)
    def _():
        greet(at_z(-1))

    @pl.when(up_ok)
    def _():
        greet(at_z(1))

    def remote(source, target, send_sem, recv_sem, device):
        return pltpu.make_async_remote_copy(
            src_ref=source, dst_ref=target, send_sem=send_sem, recv_sem=recv_sem,
            device_id=device, device_id_type=pl.DeviceIdType.MESH,
        )

    def done(ref, sem):
        pltpu.make_async_copy(ref, ref, sem).wait()


    def slot(i, f):
        if i < n:
            return held[i].at[f]
        return held[n].at[f, pl.ds(0, height), pl.ds((i - n) * half, half)]

    def spare_of(i):
        return spare[i] if i < n else spare[n].at[:, pl.ds((i - n) * half, half)]

    def across_y(i):
        return remote(spare_of(i), slot(i, me), w_y.at[i], w_recv.at[i, me], to_y)

    def along(i, f, step):
        side = 0 if step < 0 else 1
        return remote(slot(i, f), slot(i, f), w_z.at[i, f, side], w_recv.at[i, f], at_z(step))

    def send_z(i, f, step):
        @pl.when(down_ok if step < 0 else up_ok)
        def _():
            along(i, f, step).start()

    def send_both(i, f):
        for step in (-1, 1):
            send_z(i, f, step)

    def take_other(i):
        done(slot(i, other), w_recv.at[i, other])

    def take(i, d, qs=(0, 1)):
        for sign in (1, -1):
            s = z + sign * d

            @pl.when((s < outer) if sign > 0 else (s >= 0))
            def _():
                for q in qs:
                    f = s * 2 + q
                    done(slot(i, f), w_recv.at[i, f])
                    send_z(i, f, -sign)

    def pack(i):
        for yy in range(2):

            @pl.when(y == yy)
            def _():
                for to, which in ((spare[i], 1 - yy), (held[i].at[me], yy)):
                    at = 0
                    for piece in joined(raw_gate, raw_up, which, *chunks[i]):
                        to[:, at : at + piece.shape[1]] = piece.astype(to.dtype)
                        at += piece.shape[1]

    starts = [0]
    for lo, hi in chunks:
        starts.append(starts[-1] + 2 * (hi - lo))

    def pack_scale():
        tiles = 2 * height // 128
        gates, ups = (
            jnp.broadcast_to(
                jnp.concatenate([ref[pl.ds(x * tiles + i, 1)] for i in range(tiles)], 1),
                (8, 2 * height),
            )
            for ref in (gate_scale, up_scale)
        )
        for yy in range(2):

            @pl.when(y == yy)
            def _():
                at = 0
                for lo, hi in chunks:
                    for piece in joined(gates, ups, yy, lo, hi):
                        scale[:, at : at + piece.shape[1]] = piece
                        at += piece.shape[1]


    def place(cc, xx, yy):
        return cc * 4 + xx * 2 + yy

    mine, near_x, near_y, diagonal = (
        place(c, x, y), place(c, 1 - x, y), place(c, x, 1 - y), place(c, 1 - x, 1 - y)
    )
    half_rows = (rows - split) // 2
    spans = (pl.ds(0, split), pl.ds(split, half_rows), pl.ds(split + half_rows, half_rows))

    def move(t, h, device, at):
        here = allx.at[t, spans[h]]
        return remote(here, here, t_send.at[at], t_recv.at[t, h], device)

    def moved(t, h):
        done(allx.at[t, spans[h]], t_recv.at[t, h])

    def share(t, at):
        return remote(allx.at[t], allx.at[t], t_send.at[at], t_recv.at[t, 0], to_core)

    own_x = [move(mine, h, to_x, h) for h in range(3)]
    own_y = [move(mine, h, to_y, 3 + h) for h in range(3)]
    relay_y = move(near_x, 0, to_y, 6)
    relay_x = [move(near_y, 1 + i, to_x, 7 + i) for i in range(2)]
    shares = [share(t, 9 + i) for i, t in enumerate((mine, near_x, near_y, diagonal))]

    def normalize():
        step = 64 if rows % 64 == 0 else 32

        def body(i, carry):
            at = pl.ds(pl.multiple_of(i * step, step), step)
            value = raw_tok[at].astype(jnp.float32)
            size = lax.rsqrt(jnp.mean(value * value, axis=-1, keepdims=True) + 1e-06)
            allx[mine, at] = (value * size * gain[...]).astype(allx.dtype)
            return carry

        lax.fori_loop(0, rows // step, body, 0)

    def early(i, d, qs=(0, 1)):
        @pl.when(inside)
        def _():
            take(i, d, qs)

    def late(i, ds, qs=(0, 1)):
        @pl.when(jnp.logical_not(inside))
        def _():
            for d in ds:
                take(i, d, qs)

    loads[0].wait()
    loads[1].wait()
    pack(0)
    pl.semaphore_wait(
        barrier, 3 + jnp.minimum(z, 1) + jnp.minimum(outer - 1 - z, 1)
    )
    across_y(0).start()
    send_both(0, me)
    loads[2].wait()
    normalize()
    for h in range(3):
        own_x[h].start()
    own_y[1].start()
    pack(1)
    across_y(1).start()
    send_both(1, me)
    own_y[2].start()
    own_y[0].start()
    shares[0].start()
    for i in range(2, n):
        pack(i)
        across_y(i).start()
    loads[3].wait()
    for yy in range(2):

        @pl.when(y == yy)
        def _():
            spare[n][...] = raw_down[(1 - yy) * height : (2 - yy) * height].astype(spare[n].dtype)
            held[n][me, :height, :] = raw_down[yy * height : (yy + 1) * height].astype(held[n].dtype)

    for i in range(n, items):
        across_y(i).start()
    pack_scale()
    tail = held[n].shape[1] - height
    if tail:
        for f in range(2 * outer):
            held[n][f, height:, :] = jnp.zeros((tail, block), held[n].dtype)


    def silu(v):
        return v * (1.0 / (1.0 + jnp.exp(-v)))

    def store(t, both, lo, hi):
        odd = (hi - lo) % 128
        even = hi - lo - odd
        if even:
            value = silu(both[:, :even]) * both[:, even : 2 * even]
            hid[t, :, lo : lo + even] = value.astype(hid.dtype)
        if odd:
            both = both[:, 2 * even :]
            value = silu(both) * pltpu.roll(both, odd, 1)
            lane = lax.broadcasted_iota(jnp.int32, value.shape, 1)
            at = lo + even
            hid[t, :, at : at + 2 * odd] = jnp.where(lane < odd, value, 0.0).astype(hid.dtype)

    def scale_of(i):
        return scale[0:1, starts[i] : starts[i + 1]]

    def tile(k):
        j, cc = k // 2, c + (1 - 2 * c) * lax.rem(k, 2)
        return place(cc, x + (1 - 2 * x) * lax.rem(j, 2), y + (1 - 2 * y) * (j // 2))

    def hidden(i, start=0, stop=8):
        lo, hi = chunks[i]

        def body(k, carry):
            t = tile(k)
            both = jnp.dot(
                allx[t], held[i][...].reshape(depth, 2 * (hi - lo)),
                preferred_element_type=jnp.float32,
            )
            store(t, both * scale_of(i), lo, hi)
            return carry

        lax.fori_loop(start, stop, body, 0)


    deep = held[0].shape[1]
    near = jnp.where(z * 2 < outer, 0, 1)

    def reach(start, size):
        return pl.ds(pl.multiple_of(start, 2 * deep), size)

    def partly(i, t, start, planes_in):
        size = planes_in * 2 * deep
        return jnp.dot(
            allx[t, :, reach(start * 2 * deep, size)],
            held[i][pl.ds(start * 2, planes_in * 2)].reshape(size, held[i].shape[2]),
            preferred_element_type=jnp.float32,
        )

    def begin(i):
        lanes = starts[i + 1] - starts[i]

        def body(t, carry):
            early_sum[t, :, :lanes] = partly(i, t, near, outer - 1)
            return carry

        lax.fori_loop(0, 8, body, 0)

    def end(i):
        lanes = starts[i + 1] - starts[i]

        def body(t, carry):
            both = early_sum[t, :, :lanes] + partly(i, t, (1 - near) * (outer - 1), 1)
            store(t, both * scale_of(i), *chunks[i])
            return carry

        lax.fori_loop(0, 8, body, 0)


    ready = chunks[1][1]

    def head():
        f = z * 2

        def body(t, carry):
            head_sum[t] = jnp.dot(
                hid[t, :, :ready], held[n][f, :ready], preferred_element_type=jnp.float32
            )
            return carry

        lax.fori_loop(0, 8, body, 0)

    last = n - 1
    distances = range(1, outer)
    moved(near_x, 0)
    relay_y.start()
    take_other(0)
    send_both(0, other)
    early(0, 1)
    moved(near_y, 1)
    relay_x[0].start()
    take_other(1)
    send_both(1, other)
    send_both(2, me)
    early(0, 2)
    moved(near_y, 2)
    relay_x[1].start()
    early(1, 1)
    moved(near_x, 1)
    moved(near_x, 2)
    shares[1].start()
    take_other(2)
    send_both(2, other)
    moved(near_y, 0)
    shares[2].start()
    early(1, 2)
    early(2, 1)
    for k in range(3):
        t = place(1 - c, *((x, y), (1 - x, y), (x, 1 - y))[k])
        done(allx.at[t], t_recv.at[t, 0])
    late(0, distances)
    hidden(0, 0, 6)
    for h in range(3):
        moved(diagonal, h)
    shares[3].start()
    for i in range(n, items):
        take_other(i)
    early(2, 2)
    send_both(last, me)
    take_other(last)
    send_both(last, other)
    t = place(1 - c, 1 - x, 1 - y)
    done(allx.at[t], t_recv.at[t, 0])
    hidden(0, 6, 8)
    early(last, 1)
    late(1, distances)
    hidden(1)
    early(last, 2)
    for q in range(2):
        for i in range(n, items):
            send_both(i, z * 2 + q)
    head()
    for i in range(2, n):
        late(i, range(1, outer - 1))
        begin(i)
        late(i, (outer - 1,))
        end(i)


    planes = []
    for spot in range(outer):
        plane = 0
        for zz in range(outer):
            order = sorted(range(outer), key=lambda s: (abs(s - zz), -s))
            plane = plane + jnp.where(z == zz, order[spot], 0)
        planes.append(plane)
    units = units_of(outer, block)

    def high(k):
        return pl.ds(0, rows if units[k][3] == block else rows // 2)

    def send_a(k):
        wide_as = pl.ds(0, units[k][3])
        return remote(
            part.at[k % 2, pl.ds((1 - c) * 4, 4), :, wide_as], got_a.at[k, :, :, wide_as],
            a_send.at[k], a_recv.at[k], to_core,
        )

    def send_b(k):
        return [
            remote(
                sums.at[k % 3, pl.ds((1 - first) * 2, 2), high(k)], got.at[k, :, high(k)],
                b_send.at[k, i], b_recv.at[k, i], to,
            )
            for i, (sums, first, got, to) in enumerate(
                ((sum_a, x, got_ba, to_x), (sum_b, y, got_bb, to_y))
            )
        ]

    def send_c(k):
        return [
            remote(
                source.at[k % 3, high(k)], got.at[k, high(k)], c_send.at[k, i], c_recv.at[k, i], to
            )
            for i, (source, got, to) in enumerate(((next_a, got_ca, to_y), (next_b, got_cb, to_x)))
        ]

    def wide(value):
        return value.astype(jnp.float32)

    def multiply(k):
        if k >= 2:
            send_a(k - 2).wait_send()
        spot, q, lo, count = units[k]
        f = planes[spot] * 2 + q

        def body(t, carry):
            if k:
                total = jnp.dot(
                    hid[t], held[n][f, :, lo : lo + count], preferred_element_type=jnp.float32
                )
            else:
                total = head_sum[t] + jnp.dot(
                    hid[t, :, ready:], held[n][f, ready:], preferred_element_type=jnp.float32
                )
            part[k % 2, t, :, 0:count] = total.astype(part.dtype)
            return carry

        lax.fori_loop((1 - c) * 4, (1 - c) * 4 + 4, body, 0)
        send_a(k).start()
        lax.fori_loop(c * 4, c * 4 + 4, body, 0)

    def first(k):
        count = units[k][3]
        done(got_a.at[k, :, :, pl.ds(0, count)], a_recv.at[k])
        if k >= 3:
            for copy in send_b(k - 3):
                copy.wait_send()

        def body(i, carry):
            total = wide(part[k % 2, c * 4 + i, :, 0:count]) + wide(got_a[k, i, :, 0:count])
            total = total.astype(part.dtype)
            turned = lax.rem(i, 2) * 2 + i // 2
            if count == block:
                sum_a[k % 3, i] = total[:, :half]
                sum_b[k % 3, turned] = total[:, half:]
            else:
                sum_a[k % 3, i, : rows // 2] = total[: rows // 2]
                sum_b[k % 3, turned, : rows // 2] = total[rows // 2 :]
            return carry

        lax.fori_loop(0, 4, body, 0)
        for copy in send_b(k):
            copy.start()

    def second(k):
        h, s = high(k), k % 3
        for i, got in enumerate((got_ba, got_bb)):
            done(got.at[k, :, h], b_recv.at[k, i])
        if k >= 3:
            for copy in send_c(k - 3):
                copy.wait_send()
        next_a[s, h] = (wide(sum_a[s, x * 2 + 1 - y, h]) + wide(got_ba[k, 1 - y, h])).astype(next_a.dtype)
        next_b[s, h] = (wide(sum_b[s, y * 2 + 1 - x, h]) + wide(got_bb[k, 1 - x, h])).astype(next_b.dtype)
        for copy in send_c(k):
            copy.start()
        keep_a[s, h] = wide(sum_a[s, x * 2 + y, h]) + wide(got_ba[k, y, h])
        keep_b[s, h] = wide(sum_b[s, y * 2 + x, h]) + wide(got_bb[k, x, h])

    def third(k):
        h, s = high(k), k % 3
        for i, got in enumerate((got_ca, got_cb)):
            done(got.at[k, h], c_recv.at[k, i])
        spot, q, lo, count = units[k]
        base = (planes[spot] * 2 + q) * block
        for i, (keep, got) in enumerate(((keep_a, got_ca), (keep_b, got_cb))):
            if count == block:
                lead, down_rows = i * half, pl.ds(0, rows)
            else:
                lead, down_rows = lo, pl.ds(i * (rows // 2), rows // 2)
            at = pl.ds(pl.multiple_of(base + lead, half), half)
            result[down_rows, at] = ((keep[s, h] + wide(got[k, h])) * down_scale[:, at]).astype(out.dtype)

    def write(k):
        spot, q, lo, count = units[k]
        at = pl.ds(pl.multiple_of((planes[spot] * 2 + q) * block + lo, half), count)
        return pltpu.make_async_copy(result.at[:, at], out.at[:, at], raw_sem.at[k])

    def finish(k):
        third(k)
        write(k).start()

    count = len(units)
    for k in range(count):
        if 1 <= k <= 4:
            for i in range(n, items):
                early(i, (k + 1) // 2, ((k - 1) % 2,))
        spot, q, lo, size = units[k]
        if spot >= 1:
            for i in range(n, items):
                if size == block or (i - n) * half == lo:
                    late(i, (spot,), (q,))
        multiply(k)
        first(k)
        if 1 <= k < count - 2:
            second(k - 1)
        if 3 <= k < count - 1:
            finish(k - 3)
    second(count - 3)
    second(count - 2)
    finish(count - 4)
    second(count - 1)
    for i in range(items):
        across_y(i).wait_send()
        for step in (-1, 1):
            for d in range(outer):
                s = z - step * d

                @pl.when(((s < outer) & down_ok) if step < 0 else ((s >= 0) & up_ok))
                def _():
                    for q in range(2):
                        along(i, s * 2 + q, step).wait_send()

    for copy in (*own_x, *own_y, relay_y, *relay_x, *shares):
        copy.wait_send()
    for k in range(count - 3, count):
        finish(k)
    for k in range(count):
        write(k).wait()
    for k in range(count - 3, count):
        for copy in (*send_b(k), *send_c(k)):
            copy.wait_send()
    for k in range(count - 2, count):
        send_a(k).wait_send()


def fused_layer(outer, tokens, gain, gate, up, gate_scale, up_scale, down, down_scale):
    rows, depth = tokens.shape
    deep, width = gate.shape
    height, block, count = width // 4, down.shape[1], 2 * outer
    half = block // 2
    padded = -(-height // 128) * 128
    chunks = hidden_chunks(height)
    n = len(chunks)
    kind = jnp.bfloat16

    def room(*shape, dtype=kind):
        return pltpu.VMEM(shape, dtype)

    anywhere = pl.BlockSpec(memory_space=pl.ANY)
    inside = pl.BlockSpec(memory_space=pltpu.VMEM)
    dma = pltpu.SemaphoreType.DMA
    units = len(units_of(outer, block))
    return pl.pallas_call(
        functools.partial(layer_kernel, outer, chunks, rows // 96 * 16),
        out_shape=jax.ShapeDtypeStruct((rows, depth), kind),
        in_specs=[anywhere, inside, anywhere, anywhere, inside, inside, anywhere, inside],
        out_specs=anywhere,
        scratch_shapes=[
            room(rows, depth),
            room(deep, 2 * height, dtype=jnp.float32),
            room(deep, 2 * height, dtype=jnp.float32),
            room(2 * height, block, dtype=jnp.float32),
            room(8, 2 * height, dtype=jnp.float32),
            *(room(deep, 2 * (hi - lo)) for lo, hi in chunks),
            room(height, block),
            room(8, rows, depth),
            *(room(count, deep, 2 * (hi - lo)) for lo, hi in chunks),
            room(count, padded, block),
            room(8, rows, padded),
            room(2, 8, rows, block),
            room(units, 4, rows, block),
            room(3, 4, rows, half),
            room(3, 4, rows, half),
            room(units, 2, rows, half),
            room(units, 2, rows, half),
            room(3, rows, half, dtype=jnp.float32),
            room(3, rows, half, dtype=jnp.float32),
            room(3, rows, half),
            room(3, rows, half),
            room(units, rows, half),
            room(units, rows, half),
            room(rows, depth),
            room(8, rows, 256, dtype=jnp.float32),
            room(8, rows, block, dtype=jnp.float32),
            dma((max(units, 4),)),
            dma((n + 2, count)),
            dma((n + 2,)),
            dma((n + 2, count, 2)),
            dma((8, 3)),
            dma((13,)),
            dma((units,)),
            dma((units,)),
            dma((units, 2)),
            dma((units, 2)),
            dma((units, 2)),
            dma((units, 2)),
        ],
        compiler_params=pltpu.CompilerParams(
            collective_id=1, has_side_effects=True, vmem_limit_bytes=67043328
        ),
        cost_estimate=pl.CostEstimate(
            flops=48 * rows * depth * height, bytes_accessed=8 * rows * depth, transcendentals=0
        ),
    )(tokens, gain, gate, up, gate_scale, up_scale, down, down_scale)


def on_plane(
    tokens, norm_gain, gate_weight, up_weight, gate_scale, up_scale, down_weight, down_scale
):
    outer, _ = grid_of(lax.axis_size("fs"))
    return fused_layer(
        outer, tokens, norm_gain[None], gate_weight, up_weight,
        gate_scale.reshape(-1, 128), up_scale.reshape(-1, 128), down_weight, down_scale[None],
    )


def planar(mesh, tokens, gate_weight):
    sizes = mesh.shape
    if grid_of(sizes["fs"]) != (4, 2) or sizes["rep"] != 2 or sizes["tp"] != 2:
        return False
    width, rows = gate_weight.shape[1] // 8, tokens.shape[0] // mesh.size
    depth = gate_weight.shape[0]
    return (
        gate_weight.shape[1] % 8 == 0 and width % 128 == 64 and width > 256
        and rows % 96 == 0 and depth % (sizes["fs"] * 256) == 0
    )


def solution(mesh):
    placed = (
        P(("rep", "fs", "tp"), None),
        P(),
        P("fs", "tp"),
        P("fs", "tp"),
        P("tp"),
        P("tp"),
        P("tp", "fs"),
        P(),
    )

    def layer(tokens, norm_gain, gate_weight, *rest):
        return jax.shard_map(
            on_plane if planar(mesh, tokens, gate_weight) else on_device,
            mesh=mesh,
            in_specs=placed,
            out_specs=P(("rep", "fs", "tp"), None),
            check_vma=False,
        )(tokens, norm_gain, gate_weight, *rest)

    return layer
```

```python
import functools
import math

import jax
import jax.numpy as jnp
from jax import lax
from jax.experimental import pallas as pl
from jax.experimental.pallas import tpu as pltpu
from jax.sharding import PartitionSpec as P


def grid_of(count):
    inner = 1
    while (inner * 2) ** 2 <= count and count % (inner * 2) == 0:
        inner *= 2
    return count // inner, inner


def swap(x, axis):
    return lax.ppermute(x, axis, [(0, 1), (1, 0)])


def gather_kernel(outer, inner, *refs):
    local, whole = refs[:3], refs[3:6]
    own_sem, near_sem, relay_sem, cross_sem, recv_sem = refs[6:]
    me = lax.axis_index("fs")
    z, y = me // inner, lax.rem(me, inner)
    offsets = [o for o in (1, -1, 2, -2) if abs(o) < outer]

    def inside(o):
        return (z + o >= 0) & (z + o < outer)

    def peer(i):
        return z * inner + lax.rem(y + i, inner)

    barrier = pltpu.get_barrier_semaphore()
    for o in offsets:

        @pl.when(inside(o))
        def _():
            pl.semaphore_signal(
                barrier, inc=1, device_id={"fs": me + o * inner},
                device_id_type=pl.DeviceIdType.MESH,
            )

    for i in range(1, inner):
        pl.semaphore_signal(
            barrier, inc=1, device_id={"fs": peer(i)}, device_id_type=pl.DeviceIdType.MESH
        )
    reach = min(2, outer - 1)
    peers = jnp.minimum(z, reach) + jnp.minimum(outer - 1 - z, reach) + inner - 1
    pl.semaphore_wait(barrier, peers)

    def slot(a, row, column):
        return row * inner + column if a < 2 else row

    def send(a, source, row, column, target, sem):
        place = slot(a, row, column)
        return pltpu.make_async_remote_copy(
            src_ref=source,
            dst_ref=whole[a].at[place],
            send_sem=sem,
            recv_sem=recv_sem.at[a, place],
            device_id={"fs": target},
            device_id_type=pl.DeviceIdType.MESH,
        )

    def near(a, o):
        return send(a, local[a], z, y, me + o * inner, near_sem.at[a, offsets.index(o)])

    def relay(a, d):
        step = 1 if d > 0 else -1
        source = whole[a].at[slot(a, z - d, y)]
        return send(a, source, z - d, y, me + step * inner, relay_sem.at[a, outer + d])

    def cross(a, d, i):
        source = local[a] if d == 0 else whole[a].at[slot(a, z - d, y)]
        return send(a, source, z - d, y, peer(i), cross_sem.at[a, outer + d, i])

    def arrived(a, row, column):
        place = slot(a, row, column)
        return pltpu.make_async_copy(local[a], whole[a].at[place], recv_sem.at[a, place])

    def keep(a):
        return pltpu.make_async_copy(local[a], whole[a].at[slot(a, z, y)], own_sem.at[a])

    def take(a, d):
        @pl.when(inside(-d))
        def _():
            arrived(a, z - d, y).wait()
            if a < 2:
                for i in range(1, inner):
                    cross(a, d, i).start()
            if abs(d) >= 2:
                step = 1 if d > 0 else -1

                @pl.when(inside(step))
                def _():
                    relay(a, d).start()

    def open_near(a, o):
        @pl.when(inside(o))
        def _():
            near(a, o).start()

    distances = [d * sign for d in range(1, outer) for sign in (1, -1)]
    for o in offsets[:2]:
        open_near(0, o)
    for i in range(1, inner):
        cross(0, 0, i).start()
    for o in offsets[:2]:
        open_near(1, o)
    for i in range(1, inner):
        cross(1, 0, i).start()
    for a in range(2):
        for o in offsets[2:]:
            open_near(a, o)
    for a in range(3):
        keep(a).start()
    for d in distances[:4]:
        for a in range(2):
            take(a, d)
    for o in offsets:
        open_near(2, o)
    for d in distances[4:]:
        for a in range(2):
            take(a, d)
    for d in distances:
        take(2, d)

    for a in range(3):
        keep(a).wait()
        for o in offsets:

            @pl.when(inside(o))
            def _():
                near(a, o).wait_send()

        for d in distances:
            if abs(d) >= 2:

                @pl.when(inside(-d) & inside(1 if d > 0 else -1))
                def _():
                    relay(a, d).wait_send()

    for a in range(2):
        for d in [0] + distances:

            @pl.when(inside(-d))
            def _():
                for i in range(1, inner):
                    cross(a, d, i).wait_send()
                    arrived(a, z - d, lax.rem(y + i, inner)).wait()


def gather_weights(outer, inner, gate, up, down):
    shapes = [(outer * inner, *gate.shape), (outer * inner, *up.shape), (outer, *down.shape)]
    anywhere = pl.BlockSpec(memory_space=pl.ANY)
    return pl.pallas_call(
        functools.partial(gather_kernel, outer, inner),
        out_shape=[jax.ShapeDtypeStruct(shape, gate.dtype) for shape in shapes],
        in_specs=[anywhere] * 3,
        out_specs=[anywhere] * 3,
        scratch_shapes=[
            pltpu.SemaphoreType.DMA((3,)),
            pltpu.SemaphoreType.DMA((3, 4)),
            pltpu.SemaphoreType.DMA((3, 2 * outer)),
            pltpu.SemaphoreType.DMA((2, 2 * outer, inner)),
            pltpu.SemaphoreType.DMA((3, outer * inner)),
        ],
        compiler_params=pltpu.CompilerParams(collective_id=0, has_side_effects=True),
        cost_estimate=pl.CostEstimate(
            flops=0, bytes_accessed=32 * sum(math.prod(shape) for shape in shapes), transcendentals=0
        ),
    )(gate, up, down)


def roll(x, shift):
    return lax.dynamic_slice_in_dim(jnp.concatenate([x, x], -1), shift, x.shape[-1], x.ndim - 1)


def reorder(x, outer, inner, y):
    block = x.shape[-1] // (outer * inner)
    position = lax.broadcasted_iota(jnp.int32, x.shape, x.ndim - 1) % (inner * block)
    ahead = roll(x, y * block)
    behind = roll(x, (x.shape[-1] - inner * block + y * block) % x.shape[-1])
    return jnp.where(position + y * block < inner * block, ahead, behind)


def gather_rows(x, axis):
    if lax.axis_size(axis) == 2:
        return jnp.stack([x, swap(x, axis)])
    return lax.all_gather(x, axis)


def reduce_rows(x, axis):
    if lax.axis_size(axis) == 2:
        return x[0].astype(jnp.float32) + swap(x[1].astype(jnp.bfloat16), axis).astype(jnp.float32)
    return lax.psum_scatter(
        x.astype(jnp.bfloat16), axis, scatter_dimension=0, tiled=False
    ).astype(jnp.float32)


def on_device(
    tokens, norm_gain, gate_weight, up_weight, gate_scale, up_scale, down_weight, down_scale
):
    groups, count = lax.axis_size("rep"), lax.axis_size("fs")
    tps = lax.axis_size("tp")
    outer, inner = grid_of(count)
    y = lax.axis_index("fs") % inner
    width = gate_weight.shape[1] // groups
    start = lax.axis_index("rep") * width
    gate_local, up_local = (
        lax.dynamic_slice_in_dim(weight, start, width, 1).astype(jnp.bfloat16)
        for weight in (gate_weight, up_weight)
    )
    down_local = lax.dynamic_slice_in_dim(down_weight, start, width, 0).astype(jnp.bfloat16)
    gate_scale, up_scale = (
        lax.dynamic_slice_in_dim(scale, start, width, 0) for scale in (gate_scale, up_scale)
    )

    gate_whole, up_whole, down_near = gather_weights(
        outer, inner, gate_local, up_local, down_local
    )

    values = tokens.astype(jnp.float32)
    own_normed = (
        values * lax.rsqrt(jnp.mean(values * values, axis=-1, keepdims=True) + 1e-06) * norm_gain
    ).astype(jnp.bfloat16)
    rows, depth = own_normed.shape
    normed = gather_rows(gather_rows(own_normed, "tp"), "rep").swapaxes(0, 1).reshape(-1, depth)

    gate_whole, up_whole = gate_whole.reshape(depth, width), up_whole.reshape(depth, width)
    cuts = [slice(0, outer // 2), slice(outer // 2, outer)] if outer > 1 else [slice(0, 1)]
    pieces = [down_near[cut] for cut in cuts]
    for i in range(1, inner):
        pairs = [(f, f - f % inner + (f - i) % inner) for f in range(count)]
        pieces += [lax.ppermute(down_near[cut], "fs", pairs) for cut in cuts]
    gate_value = jnp.dot(normed, gate_whole, preferred_element_type=jnp.float32)
    up_value = jnp.dot(normed, up_whole, preferred_element_type=jnp.float32)
    hidden = (jax.nn.silu(gate_value * gate_scale) * (up_value * up_scale)).astype(jnp.bfloat16)

    near = len(cuts)
    later, pieces[near:] = lax.optimization_barrier((hidden, pieces[near:]))
    block = down_local.shape[1]
    columns = []
    for at, piece in enumerate(pieces):
        partial_value = jnp.dot(
            hidden if at < near else later, jnp.concatenate(list(piece), 1), preferred_element_type=jnp.float32
        ).astype(jnp.bfloat16)
        partial_value = partial_value.reshape(tps, groups, rows, -1)
        total = reduce_rows(reduce_rows(partial_value, "tp"), "rep")
        columns += [total[:, c * block : (c + 1) * block] for c in range(len(piece))]
    summed = jnp.concatenate([columns[i * outer + a] for a in range(outer) for i in range(inner)], -1)
    scale = reorder(down_scale[None], outer, inner, y)
    mixed = (summed * scale).astype(jnp.bfloat16)
    return reorder(mixed, outer, inner, (inner - y) % inner)


def hidden_chunks(width):
    whole = width // 128 * 128
    return [(0, whole - 256), (whole - 256, whole - 128), (whole, width), (whole - 128, whole)]


def columns(value, at, count):
    shift = at % 128
    if shift == 0:
        return value[:, at : at + count]
    low, high = at - shift, min(at - shift + count + 128, value.shape[1])
    return pltpu.roll(value[:, low:high], high - low - shift, 1)[:, :count]


def joined(gate, up, part, lo, hi):
    at = part * (gate.shape[1] // 2) + lo
    odd = (hi - lo) % 128
    even = hi - lo - odd
    pieces = [columns(gate, at, even), columns(up, at, even)] if even else []
    if odd:
        left = columns(gate, at + even, 128)
        right = pltpu.roll(columns(up, at + even, 128), odd, 1)
        lane = lax.broadcasted_iota(jnp.int32, left.shape, 1)
        pieces.append(jnp.where(lane < odd, left, right))
    return pieces


def units_of(outer, block):
    units = [(k // 2, k % 2, 0, block) for k in range(2 * outer - 1)]
    half = block // 2
    return units + [(outer - 1, 1, 0, half), (outer - 1, 1, half, half)]


def layer_kernel(outer, chunks, split, *refs):
    n = len(chunks)
    tokens, gain, gate, up, gate_scale, up_scale, down, down_scale, out = refs[:9]
    refs = refs[9:]
    raw_tok, raw_gate, raw_up, raw_down, scale = refs[:5]
    spare, allx, held, hid, part = refs[5 : n + 6], refs[n + 6], refs[n + 7 : 2 * n + 8], *refs[2 * n + 8 : 2 * n + 10]
    refs = refs[2 * n + 10 :]
    got_a, sum_a, sum_b, got_ba, got_bb, keep_a, keep_b, next_a, next_b, got_ca, got_cb, result, early_sum, head_sum = refs[:14]
    (
        raw_sem, w_recv, w_y, w_z, t_recv, t_send,
        a_send, a_recv, b_send, b_recv, c_send, c_recv,
    ) = refs[14:]
    items = n + 2
    x, me, c = lax.axis_index("rep"), lax.axis_index("fs"), lax.axis_index("tp")
    z, y = me // 2, lax.rem(me, 2)
    other = z * 2 + 1 - y
    rows, depth = raw_tok.shape
    height, block = spare[n].shape
    half = block // 2
    to_core, to_x, to_y = {"tp": 1 - c}, {"rep": 1 - x}, {"fs": other}
    up_ok, down_ok = z + 1 < outer, z > 0
    inside = down_ok & up_ok

    def at_z(step):
        return {"fs": me + 2 * step}

    span = pl.ds(pl.multiple_of(x * (2 * height), 128), 2 * height)
    low = height // 128 * 128
    own_part, other_part = (y * low, low + 128), ((1 - y) * (low + 128), low)

    def load_columns(source, target, part, at):
        lead, size = part
        return pltpu.make_async_copy(
            source.at[:, pl.ds(pl.multiple_of(x * (2 * height) + lead, 128), size)],
            target.at[:, pl.ds(pl.multiple_of(lead, 128), size)],
            raw_sem.at[at],
        )

    own_loads = [load_columns(gate, raw_gate, own_part, 0), load_columns(up, raw_up, own_part, 1)]
    other_loads = [
        load_columns(gate, raw_gate, other_part, 2), load_columns(up, raw_up, other_part, 3),
    ]
    late_loads = [
        pltpu.make_async_copy(tokens, raw_tok, raw_sem.at[4]),
        pltpu.make_async_copy(down.at[span], raw_down, raw_sem.at[5]),
    ]
    for load in (*own_loads, *other_loads, *late_loads):
        load.start()

    barrier = pltpu.get_barrier_semaphore()

    def greet(target):
        pl.semaphore_signal(
            barrier, inc=1, device_id=target, device_id_type=pl.DeviceIdType.MESH
        )

    for target in (to_core, to_x, to_y):
        greet(target)

    @pl.when(down_ok)
    def _():
        greet(at_z(-1))

    @pl.when(up_ok)
    def _():
        greet(at_z(1))

    def remote(source, target, send_sem, recv_sem, device):
        return pltpu.make_async_remote_copy(
            src_ref=source, dst_ref=target, send_sem=send_sem, recv_sem=recv_sem,
            device_id=device, device_id_type=pl.DeviceIdType.MESH,
        )

    def done(ref, sem):
        pltpu.make_async_copy(ref, ref, sem).wait()


    def slot(i, f):
        if i < n:
            return held[i].at[f]
        return held[n].at[f, pl.ds(0, height), pl.ds((i - n) * half, half)]

    def spare_of(i):
        return spare[i] if i < n else spare[n].at[:, pl.ds((i - n) * half, half)]

    def across_y(i):
        return remote(spare_of(i), slot(i, me), w_y.at[i], w_recv.at[i, me], to_y)

    def along(i, f, step):
        side = 0 if step < 0 else 1
        return remote(slot(i, f), slot(i, f), w_z.at[i, side], w_recv.at[i, f], at_z(step))

    def send_z(i, f, step):
        @pl.when(down_ok if step < 0 else up_ok)
        def _():
            along(i, f, step).start()

    def send_both(i, f):
        for step in (-1, 1):
            send_z(i, f, step)

    def take_other(i):
        done(slot(i, other), w_recv.at[i, other])

    def take(i, d, qs=(0, 1)):
        for sign in (1, -1):
            s = z + sign * d

            @pl.when((s < outer) if sign > 0 else (s >= 0))
            def _():
                for q in qs:
                    f = s * 2 + q
                    done(slot(i, f), w_recv.at[i, f])
                    send_z(i, f, -sign)

    def pack(i, sides=(0, 1)):
        for yy in range(2):

            @pl.when(y == yy)
            def _():
                for to, which in [((held[i].at[me], yy), (spare[i], 1 - yy))[side] for side in sides]:
                    at = 0
                    for piece in joined(raw_gate, raw_up, which, *chunks[i]):
                        to[:, at : at + piece.shape[1]] = piece.astype(to.dtype)
                        at += piece.shape[1]

    starts = [0]
    for lo, hi in chunks:
        starts.append(starts[-1] + 2 * (hi - lo))

    def pack_scale():
        tiles = 2 * height // 128
        gates, ups = (
            jnp.broadcast_to(
                jnp.concatenate([ref[pl.ds(x * tiles + i, 1)] for i in range(tiles)], 1),
                (8, 2 * height),
            )
            for ref in (gate_scale, up_scale)
        )
        for yy in range(2):

            @pl.when(y == yy)
            def _():
                at = 0
                for lo, hi in chunks:
                    for piece in joined(gates, ups, yy, lo, hi):
                        scale[:, at : at + piece.shape[1]] = piece
                        at += piece.shape[1]


    def place(cc, xx, yy):
        return cc * 4 + xx * 2 + yy

    mine, near_x, near_y, diagonal = (
        place(c, x, y), place(c, 1 - x, y), place(c, x, 1 - y), place(c, 1 - x, 1 - y)
    )
    half_rows = (rows - split) // 2
    spans = (pl.ds(0, split), pl.ds(split, half_rows), pl.ds(split + half_rows, half_rows))

    def move(t, h, device, at, seen_as):
        here = allx.at[t, spans[h]]
        return remote(here, here, t_send.at[at], t_recv.at[3 * seen_as + h], device)

    def moved(t, h, seen_as):
        done(allx.at[t, spans[h]], t_recv.at[3 * seen_as + h])

    def share(t, at):
        return remote(allx.at[t], allx.at[t], t_send.at[at], t_recv.at[at], to_core)

    own_x = [move(mine, h, to_x, h, 0) for h in range(3)]
    own_y = [move(mine, h, to_y, 3 + h, 1) for h in range(3)]
    relay_y = move(near_x, 0, to_y, 6, 2)
    relay_x = [move(near_y, 1 + i, to_x, 7 + i, 2) for i in range(2)]
    shares = [share(t, 9 + i) for i, t in enumerate((mine, near_x, near_y, diagonal))]

    def normalize():
        step = 64 if rows % 64 == 0 else 32

        def body(i, carry):
            at = pl.ds(pl.multiple_of(i * step, step), step)
            value = raw_tok[at].astype(jnp.float32)
            size = lax.rsqrt(jnp.mean(value * value, axis=-1, keepdims=True) + 1e-06)
            allx[mine, at] = (value * size * gain[...]).astype(allx.dtype)
            return carry

        lax.fori_loop(0, rows // step, body, 0)

    def early(i, d, qs=(0, 1)):
        @pl.when(inside)
        def _():
            take(i, d, qs)

    def late(i, ds, qs=(0, 1)):
        @pl.when(jnp.logical_not(inside))
        def _():
            for d in ds:
                take(i, d, qs)

    for load in own_loads:
        load.wait()
    pack(0, (0,))
    pl.semaphore_wait(
        barrier, 3 + jnp.minimum(z, 1) + jnp.minimum(outer - 1 - z, 1)
    )
    send_both(0, me)
    for load in other_loads:
        load.wait()
    pack(0, (1,))
    across_y(0).start()
    late_loads[0].wait()
    normalize()
    for h in range(3):
        own_x[h].start()
    own_y[1].start()
    pack(1)
    across_y(1).start()
    send_both(1, me)
    own_y[2].start()
    own_y[0].start()
    shares[0].start()
    for i in range(2, n):
        pack(i)
        across_y(i).start()
    late_loads[1].wait()
    for yy in range(2):

        @pl.when(y == yy)
        def _():
            spare[n][...] = raw_down[(1 - yy) * height : (2 - yy) * height].astype(spare[n].dtype)
            held[n][me, :height, :] = raw_down[yy * height : (yy + 1) * height].astype(held[n].dtype)

    for i in range(n, items):
        across_y(i).start()
    pack_scale()
    tail = held[n].shape[1] - height
    if tail:
        for f in range(2 * outer):
            held[n][f, height:, :] = jnp.zeros((tail, block), held[n].dtype)


    def silu(v):
        return v * (1.0 / (1.0 + jnp.exp(-v)))

    def store(t, both, lo, hi):
        odd = (hi - lo) % 128
        even = hi - lo - odd
        if even:
            value = silu(both[:, :even]) * both[:, even : 2 * even]
            hid[t, :, lo : lo + even] = value.astype(hid.dtype)
        if odd:
            both = both[:, 2 * even :]
            value = silu(both) * pltpu.roll(both, odd, 1)
            lane = lax.broadcasted_iota(jnp.int32, value.shape, 1)
            at = lo + even
            hid[t, :, at : at + 2 * odd] = jnp.where(lane < odd, value, 0.0).astype(hid.dtype)

    def scale_of(i):
        return scale[0:1, starts[i] : starts[i + 1]]

    def tile(k):
        j, cc = k // 2, c + (1 - 2 * c) * lax.rem(k, 2)
        return place(cc, x + (1 - 2 * x) * lax.rem(j, 2), y + (1 - 2 * y) * (j // 2))

    def hidden(i, start=0, stop=8):
        lo, hi = chunks[i]

        def body(k, carry):
            t = tile(k)
            both = jnp.dot(
                allx[t], held[i][...].reshape(depth, 2 * (hi - lo)),
                preferred_element_type=jnp.float32,
            )
            store(t, both * scale_of(i), lo, hi)
            return carry

        lax.fori_loop(start, stop, body, 0)


    deep = held[0].shape[1]
    near = jnp.where(z * 2 < outer, 0, 1)

    def reach(start, size):
        return pl.ds(pl.multiple_of(start, 2 * deep), size)

    def partly(i, t, start, planes_in):
        size = planes_in * 2 * deep
        return jnp.dot(
            allx[t, :, reach(start * 2 * deep, size)],
            held[i][pl.ds(start * 2, planes_in * 2)].reshape(size, held[i].shape[2]),
            preferred_element_type=jnp.float32,
        )

    def begin(i):
        lanes = starts[i + 1] - starts[i]

        def body(t, carry):
            early_sum[t, :, :lanes] = partly(i, t, near, outer - 1)
            return carry

        lax.fori_loop(0, 8, body, 0)

    def end(i):
        lanes = starts[i + 1] - starts[i]

        def body(t, carry):
            both = early_sum[t, :, :lanes] + partly(i, t, (1 - near) * (outer - 1), 1)
            store(t, both * scale_of(i), *chunks[i])
            return carry

        lax.fori_loop(0, 8, body, 0)


    ready = chunks[1][1]

    def head():
        f = z * 2

        def body(t, carry):
            head_sum[t] = jnp.dot(
                hid[t, :, :ready], held[n][f, :ready], preferred_element_type=jnp.float32
            )
            return carry

        lax.fori_loop(0, 8, body, 0)

    last = n - 1
    distances = range(1, outer)
    moved(near_x, 0, 0)
    relay_y.start()
    take_other(0)
    send_both(0, other)
    early(0, 1)
    moved(near_y, 1, 1)
    relay_x[0].start()
    take_other(1)
    send_both(1, other)
    send_both(2, me)
    early(0, 2)
    moved(near_y, 2, 1)
    relay_x[1].start()
    early(1, 1)
    moved(near_x, 1, 0)
    moved(near_x, 2, 0)
    shares[1].start()
    take_other(2)
    send_both(2, other)
    moved(near_y, 0, 1)
    shares[2].start()
    early(1, 2)
    early(2, 1)
    for k in range(3):
        t = place(1 - c, *((x, y), (1 - x, y), (x, 1 - y))[k])
        done(allx.at[t], t_recv.at[9 + k])
    late(0, distances)
    hidden(0, 0, 6)
    for h in range(3):
        moved(diagonal, h, 2)
    shares[3].start()
    for i in range(n, items):
        take_other(i)
    early(2, 2)
    send_both(last, me)
    take_other(last)
    send_both(last, other)
    t = place(1 - c, 1 - x, 1 - y)
    done(allx.at[t], t_recv.at[12])
    hidden(0, 6, 8)
    early(last, 1)
    late(1, distances)
    hidden(1)
    early(last, 2)
    for q in range(2):
        for i in range(n, items):
            send_both(i, z * 2 + q)
    head()
    for i in range(2, n):
        late(i, range(1, outer - 1))
        begin(i)
        late(i, (outer - 1,))
        end(i)


    planes = []
    for spot in range(outer):
        plane = 0
        for zz in range(outer):
            order = sorted(range(outer), key=lambda s: (abs(s - zz), -s))
            plane = plane + jnp.where(z == zz, order[spot], 0)
        planes.append(plane)
    units = units_of(outer, block)

    def high(k):
        return pl.ds(0, rows if units[k][3] == block else rows // 2)

    def send_a(k):
        wide_as = pl.ds(0, units[k][3])
        return remote(
            part.at[k % 2, pl.ds((1 - c) * 4, 4), :, wide_as], got_a.at[k, :, :, wide_as],
            a_send.at[k % 2], a_recv.at[k], to_core,
        )

    def send_b(k):
        return [
            remote(
                sums.at[k % 3, pl.ds((1 - first) * 2, 2), high(k)], got.at[k, :, high(k)],
                b_send.at[k % 3, i], b_recv.at[k, i], to,
            )
            for i, (sums, first, got, to) in enumerate(
                ((sum_a, x, got_ba, to_x), (sum_b, y, got_bb, to_y))
            )
        ]

    def send_c(k):
        return [
            remote(
                source.at[k % 3, high(k)], got.at[k, high(k)], c_send.at[k % 3, i], c_recv.at[k, i], to
            )
            for i, (source, got, to) in enumerate(((next_a, got_ca, to_y), (next_b, got_cb, to_x)))
        ]

    def wide(value):
        return value.astype(jnp.float32)

    def multiply(k):
        if k >= 2:
            send_a(k - 2).wait_send()
        spot, q, lo, count = units[k]
        f = planes[spot] * 2 + q

        def body(t, carry):
            if k:
                total = jnp.dot(
                    hid[t], held[n][f, :, lo : lo + count], preferred_element_type=jnp.float32
                )
            else:
                total = head_sum[t] + jnp.dot(
                    hid[t, :, ready:], held[n][f, ready:], preferred_element_type=jnp.float32
                )
            part[k % 2, t, :, 0:count] = total.astype(part.dtype)
            return carry

        lax.fori_loop((1 - c) * 4, (1 - c) * 4 + 4, body, 0)
        send_a(k).start()
        lax.fori_loop(c * 4, c * 4 + 4, body, 0)

    def first(k):
        count = units[k][3]
        done(got_a.at[k, :, :, pl.ds(0, count)], a_recv.at[k])
        if k >= 3:
            for copy in send_b(k - 3):
                copy.wait_send()

        def body(i, carry):
            total = wide(part[k % 2, c * 4 + i, :, 0:count]) + wide(got_a[k, i, :, 0:count])
            total = total.astype(part.dtype)
            turned = lax.rem(i, 2) * 2 + i // 2
            if count == block:
                sum_a[k % 3, i] = total[:, :half]
                sum_b[k % 3, turned] = total[:, half:]
            else:
                sum_a[k % 3, i, : rows // 2] = total[: rows // 2]
                sum_b[k % 3, turned, : rows // 2] = total[rows // 2 :]
            return carry

        lax.fori_loop(0, 4, body, 0)
        for copy in send_b(k):
            copy.start()

    def second(k):
        h, s = high(k), k % 3
        for i, got in enumerate((got_ba, got_bb)):
            done(got.at[k, :, h], b_recv.at[k, i])
        if k >= 3:
            for copy in send_c(k - 3):
                copy.wait_send()
        next_a[s, h] = (wide(sum_a[s, x * 2 + 1 - y, h]) + wide(got_ba[k, 1 - y, h])).astype(next_a.dtype)
        next_b[s, h] = (wide(sum_b[s, y * 2 + 1 - x, h]) + wide(got_bb[k, 1 - x, h])).astype(next_b.dtype)
        for copy in send_c(k):
            copy.start()
        keep_a[s, h] = wide(sum_a[s, x * 2 + y, h]) + wide(got_ba[k, y, h])
        keep_b[s, h] = wide(sum_b[s, y * 2 + x, h]) + wide(got_bb[k, x, h])

    def third(k):
        h, s = high(k), k % 3
        for i, got in enumerate((got_ca, got_cb)):
            done(got.at[k, h], c_recv.at[k, i])
        spot, q, lo, count = units[k]
        base = (planes[spot] * 2 + q) * block
        for i, (keep, got) in enumerate(((keep_a, got_ca), (keep_b, got_cb))):
            if count == block:
                lead, down_rows = i * half, pl.ds(0, rows)
            else:
                lead, down_rows = lo, pl.ds(i * (rows // 2), rows // 2)
            at = pl.ds(pl.multiple_of(base + lead, half), half)
            result[down_rows, at] = ((keep[s, h] + wide(got[k, h])) * down_scale[:, at]).astype(out.dtype)

    def write(k):
        spot, q, lo, count = units[k]
        at = pl.ds(pl.multiple_of((planes[spot] * 2 + q) * block + lo, half), count)
        return pltpu.make_async_copy(result.at[:, at], out.at[:, at], raw_sem.at[k])

    def finish(k):
        third(k)
        write(k).start()

    count = len(units)
    for k in range(count):
        if 1 <= k <= 4:
            for i in range(n, items):
                early(i, (k + 1) // 2, ((k - 1) % 2,))
        spot, q, lo, size = units[k]
        if spot >= 1:
            for i in range(n, items):
                if size == block or (i - n) * half == lo:
                    late(i, (spot,), (q,))
        multiply(k)
        first(k)
        if 1 <= k < count - 2:
            second(k - 1)
        if 3 <= k < count - 1:
            finish(k - 3)
    second(count - 3)
    second(count - 2)
    finish(count - 4)
    second(count - 1)
    def sent(i, planes_sent, side):
        many = pl.ds(0, 2 * planes_sent)
        if i < n:
            done(held[i].at[many], w_z.at[i, side])
        else:
            lanes = pl.ds((i - n) * half, half)
            done(held[n].at[many, pl.ds(0, height), lanes], w_z.at[i, side])

    for i in range(items):
        across_y(i).wait_send()
    for zz in range(outer):

        @pl.when(z == zz)
        def _():
            for i in range(items):
                if zz > 0:
                    sent(i, outer - zz, 0)
                if zz + 1 < outer:
                    sent(i, zz + 1, 1)

    for copy in (*own_x, *own_y, relay_y, *relay_x, *shares):
        copy.wait_send()
    for k in range(count - 3, count):
        finish(k)
    for k in range(count):
        write(k).wait()
    for k in range(count - 3, count):
        for copy in (*send_b(k), *send_c(k)):
            copy.wait_send()
    for k in range(count - 2, count):
        send_a(k).wait_send()


def fused_layer(outer, tokens, gain, gate, up, gate_scale, up_scale, down, down_scale):
    rows, depth = tokens.shape
    deep, width = gate.shape
    height, block, count = width // 4, down.shape[1], 2 * outer
    half = block // 2
    padded = -(-height // 128) * 128
    chunks = hidden_chunks(height)
    n = len(chunks)
    kind = jnp.bfloat16

    def room(*shape, dtype=kind):
        return pltpu.VMEM(shape, dtype)

    anywhere = pl.BlockSpec(memory_space=pl.ANY)
    inside = pl.BlockSpec(memory_space=pltpu.VMEM)
    dma = pltpu.SemaphoreType.DMA
    units = len(units_of(outer, block))
    return pl.pallas_call(
        functools.partial(layer_kernel, outer, chunks, rows // 96 * 16),
        out_shape=jax.ShapeDtypeStruct((rows, depth), kind),
        in_specs=[anywhere, inside, anywhere, anywhere, inside, inside, anywhere, inside],
        out_specs=anywhere,
        scratch_shapes=[
            room(rows, depth),
            room(deep, 2 * height, dtype=jnp.float32),
            room(deep, 2 * height, dtype=jnp.float32),
            room(2 * height, block, dtype=jnp.float32),
            room(8, 2 * height, dtype=jnp.float32),
            *(room(deep, 2 * (hi - lo)) for lo, hi in chunks),
            room(height, block),
            room(8, rows, depth),
            *(room(count, deep, 2 * (hi - lo)) for lo, hi in chunks),
            room(count, padded, block),
            room(8, rows, padded),
            room(2, 8, rows, block),
            room(units, 4, rows, block),
            room(3, 4, rows, half),
            room(3, 4, rows, half),
            room(units, 2, rows, half),
            room(units, 2, rows, half),
            room(3, rows, half, dtype=jnp.float32),
            room(3, rows, half, dtype=jnp.float32),
            room(3, rows, half),
            room(3, rows, half),
            room(units, rows, half),
            room(units, rows, half),
            room(rows, depth),
            room(8, rows, 256, dtype=jnp.float32),
            room(8, rows, block, dtype=jnp.float32),
            dma((max(units, 6),)),
            dma((n + 2, count)),
            dma((n + 2,)),
            dma((n + 2, 2)),
            dma((13,)),
            dma((13,)),
            dma((2,)),
            dma((units,)),
            dma((3, 2)),
            dma((units, 2)),
            dma((3, 2)),
            dma((units, 2)),
        ],
        compiler_params=pltpu.CompilerParams(
            collective_id=1, has_side_effects=True, vmem_limit_bytes=67043328
        ),
        cost_estimate=pl.CostEstimate(
            flops=48 * rows * depth * height, bytes_accessed=8 * rows * depth, transcendentals=0
        ),
    )(tokens, gain, gate, up, gate_scale, up_scale, down, down_scale)


def on_plane(
    tokens, norm_gain, gate_weight, up_weight, gate_scale, up_scale, down_weight, down_scale
):
    outer, _ = grid_of(lax.axis_size("fs"))
    return fused_layer(
        outer, tokens, norm_gain[None], gate_weight, up_weight,
        gate_scale.reshape(-1, 128), up_scale.reshape(-1, 128), down_weight, down_scale[None],
    )


def planar(mesh, tokens, gate_weight):
    sizes = mesh.shape
    if grid_of(sizes["fs"]) != (4, 2) or sizes["rep"] != 2 or sizes["tp"] != 2:
        return False
    width, rows = gate_weight.shape[1] // 8, tokens.shape[0] // mesh.size
    depth = gate_weight.shape[0]
    return (
        gate_weight.shape[1] % 8 == 0 and width % 128 == 64 and width > 256
        and rows % 96 == 0 and depth % (sizes["fs"] * 256) == 0
    )


def solution(mesh):
    placed = (
        P(("rep", "fs", "tp"), None),
        P(),
        P("fs", "tp"),
        P("fs", "tp"),
        P("tp"),
        P("tp"),
        P("tp", "fs"),
        P(),
    )

    def layer(tokens, norm_gain, gate_weight, *rest):
        return jax.shard_map(
            on_plane if planar(mesh, tokens, gate_weight) else on_device,
            mesh=mesh,
            in_specs=placed,
            out_specs=P(("rep", "fs", "tp"), None),
            check_vma=False,
        )(tokens, norm_gain, gate_weight, *rest)

    return layer
```

```python
import functools
import math

import jax
import jax.numpy as jnp
from jax import lax
from jax.experimental import pallas as pl
from jax.experimental.pallas import tpu as pltpu
from jax.sharding import PartitionSpec as P


def grid_of(count):
    inner = 1
    while (inner * 2) ** 2 <= count and count % (inner * 2) == 0:
        inner *= 2
    return count // inner, inner


def swap(x, axis):
    return lax.ppermute(x, axis, [(0, 1), (1, 0)])


def gather_kernel(outer, inner, *refs):
    local, whole = refs[:3], refs[3:6]
    own_sem, near_sem, relay_sem, cross_sem, recv_sem = refs[6:]
    me = lax.axis_index("fs")
    z, y = me // inner, lax.rem(me, inner)
    offsets = [o for o in (1, -1, 2, -2) if abs(o) < outer]

    def inside(o):
        return (z + o >= 0) & (z + o < outer)

    def peer(i):
        return z * inner + lax.rem(y + i, inner)

    barrier = pltpu.get_barrier_semaphore()
    for o in offsets:

        @pl.when(inside(o))
        def _():
            pl.semaphore_signal(
                barrier, inc=1, device_id={"fs": me + o * inner},
                device_id_type=pl.DeviceIdType.MESH,
            )

    for i in range(1, inner):
        pl.semaphore_signal(
            barrier, inc=1, device_id={"fs": peer(i)}, device_id_type=pl.DeviceIdType.MESH
        )
    reach = min(2, outer - 1)
    peers = jnp.minimum(z, reach) + jnp.minimum(outer - 1 - z, reach) + inner - 1
    pl.semaphore_wait(barrier, peers)

    def slot(a, row, column):
        return row * inner + column if a < 2 else row

    def send(a, source, row, column, target, sem):
        place = slot(a, row, column)
        return pltpu.make_async_remote_copy(
            src_ref=source,
            dst_ref=whole[a].at[place],
            send_sem=sem,
            recv_sem=recv_sem.at[a, place],
            device_id={"fs": target},
            device_id_type=pl.DeviceIdType.MESH,
        )

    def near(a, o):
        return send(a, local[a], z, y, me + o * inner, near_sem.at[a, offsets.index(o)])

    def relay(a, d):
        step = 1 if d > 0 else -1
        source = whole[a].at[slot(a, z - d, y)]
        return send(a, source, z - d, y, me + step * inner, relay_sem.at[a, outer + d])

    def cross(a, d, i):
        source = local[a] if d == 0 else whole[a].at[slot(a, z - d, y)]
        return send(a, source, z - d, y, peer(i), cross_sem.at[a, outer + d, i])

    def arrived(a, row, column):
        place = slot(a, row, column)
        return pltpu.make_async_copy(local[a], whole[a].at[place], recv_sem.at[a, place])

    def keep(a):
        return pltpu.make_async_copy(local[a], whole[a].at[slot(a, z, y)], own_sem.at[a])

    def take(a, d):
        @pl.when(inside(-d))
        def _():
            arrived(a, z - d, y).wait()
            if a < 2:
                for i in range(1, inner):
                    cross(a, d, i).start()
            if abs(d) >= 2:
                step = 1 if d > 0 else -1

                @pl.when(inside(step))
                def _():
                    relay(a, d).start()

    def open_near(a, o):
        @pl.when(inside(o))
        def _():
            near(a, o).start()

    distances = [d * sign for d in range(1, outer) for sign in (1, -1)]
    for o in offsets[:2]:
        open_near(0, o)
    for i in range(1, inner):
        cross(0, 0, i).start()
    for o in offsets[:2]:
        open_near(1, o)
    for i in range(1, inner):
        cross(1, 0, i).start()
    for a in range(2):
        for o in offsets[2:]:
            open_near(a, o)
    for a in range(3):
        keep(a).start()
    for d in distances[:4]:
        for a in range(2):
            take(a, d)
    for o in offsets:
        open_near(2, o)
    for d in distances[4:]:
        for a in range(2):
            take(a, d)
    for d in distances:
        take(2, d)

    for a in range(3):
        keep(a).wait()
        for o in offsets:

            @pl.when(inside(o))
            def _():
                near(a, o).wait_send()

        for d in distances:
            if abs(d) >= 2:

                @pl.when(inside(-d) & inside(1 if d > 0 else -1))
                def _():
                    relay(a, d).wait_send()

    for a in range(2):
        for d in [0] + distances:

            @pl.when(inside(-d))
            def _():
                for i in range(1, inner):
                    cross(a, d, i).wait_send()
                    arrived(a, z - d, lax.rem(y + i, inner)).wait()


def gather_weights(outer, inner, gate, up, down):
    shapes = [(outer * inner, *gate.shape), (outer * inner, *up.shape), (outer, *down.shape)]
    anywhere = pl.BlockSpec(memory_space=pl.ANY)
    return pl.pallas_call(
        functools.partial(gather_kernel, outer, inner),
        out_shape=[jax.ShapeDtypeStruct(shape, gate.dtype) for shape in shapes],
        in_specs=[anywhere] * 3,
        out_specs=[anywhere] * 3,
        scratch_shapes=[
            pltpu.SemaphoreType.DMA((3,)),
            pltpu.SemaphoreType.DMA((3, 4)),
            pltpu.SemaphoreType.DMA((3, 2 * outer)),
            pltpu.SemaphoreType.DMA((2, 2 * outer, inner)),
            pltpu.SemaphoreType.DMA((3, outer * inner)),
        ],
        compiler_params=pltpu.CompilerParams(collective_id=0, has_side_effects=True),
        cost_estimate=pl.CostEstimate(
            flops=0, bytes_accessed=32 * sum(math.prod(shape) for shape in shapes), transcendentals=0
        ),
    )(gate, up, down)


def roll(x, shift):
    return lax.dynamic_slice_in_dim(jnp.concatenate([x, x], -1), shift, x.shape[-1], x.ndim - 1)


def reorder(x, outer, inner, y):
    block = x.shape[-1] // (outer * inner)
    position = lax.broadcasted_iota(jnp.int32, x.shape, x.ndim - 1) % (inner * block)
    ahead = roll(x, y * block)
    behind = roll(x, (x.shape[-1] - inner * block + y * block) % x.shape[-1])
    return jnp.where(position + y * block < inner * block, ahead, behind)


def gather_rows(x, axis):
    if lax.axis_size(axis) == 2:
        return jnp.stack([x, swap(x, axis)])
    return lax.all_gather(x, axis)


def reduce_rows(x, axis):
    if lax.axis_size(axis) == 2:
        return x[0].astype(jnp.float32) + swap(x[1].astype(jnp.bfloat16), axis).astype(jnp.float32)
    return lax.psum_scatter(
        x.astype(jnp.bfloat16), axis, scatter_dimension=0, tiled=False
    ).astype(jnp.float32)


def on_device(
    tokens, norm_gain, gate_weight, up_weight, gate_scale, up_scale, down_weight, down_scale
):
    groups, count = lax.axis_size("rep"), lax.axis_size("fs")
    tps = lax.axis_size("tp")
    outer, inner = grid_of(count)
    y = lax.axis_index("fs") % inner
    width = gate_weight.shape[1] // groups
    start = lax.axis_index("rep") * width
    gate_local, up_local = (
        lax.dynamic_slice_in_dim(weight, start, width, 1).astype(jnp.bfloat16)
        for weight in (gate_weight, up_weight)
    )
    down_local = lax.dynamic_slice_in_dim(down_weight, start, width, 0).astype(jnp.bfloat16)
    gate_scale, up_scale = (
        lax.dynamic_slice_in_dim(scale, start, width, 0) for scale in (gate_scale, up_scale)
    )

    gate_whole, up_whole, down_near = gather_weights(
        outer, inner, gate_local, up_local, down_local
    )

    values = tokens.astype(jnp.float32)
    own_normed = (
        values * lax.rsqrt(jnp.mean(values * values, axis=-1, keepdims=True) + 1e-06) * norm_gain
    ).astype(jnp.bfloat16)
    rows, depth = own_normed.shape
    normed = gather_rows(gather_rows(own_normed, "tp"), "rep").swapaxes(0, 1).reshape(-1, depth)

    gate_whole, up_whole = gate_whole.reshape(depth, width), up_whole.reshape(depth, width)
    cuts = [slice(0, outer // 2), slice(outer // 2, outer)] if outer > 1 else [slice(0, 1)]
    pieces = [down_near[cut] for cut in cuts]
    for i in range(1, inner):
        pairs = [(f, f - f % inner + (f - i) % inner) for f in range(count)]
        pieces += [lax.ppermute(down_near[cut], "fs", pairs) for cut in cuts]
    gate_value = jnp.dot(normed, gate_whole, preferred_element_type=jnp.float32)
    up_value = jnp.dot(normed, up_whole, preferred_element_type=jnp.float32)
    hidden = (jax.nn.silu(gate_value * gate_scale) * (up_value * up_scale)).astype(jnp.bfloat16)

    near = len(cuts)
    later, pieces[near:] = lax.optimization_barrier((hidden, pieces[near:]))
    block = down_local.shape[1]
    columns = []
    for at, piece in enumerate(pieces):
        partial_value = jnp.dot(
            hidden if at < near else later, jnp.concatenate(list(piece), 1), preferred_element_type=jnp.float32
        ).astype(jnp.bfloat16)
        partial_value = partial_value.reshape(tps, groups, rows, -1)
        total = reduce_rows(reduce_rows(partial_value, "tp"), "rep")
        columns += [total[:, c * block : (c + 1) * block] for c in range(len(piece))]
    summed = jnp.concatenate([columns[i * outer + a] for a in range(outer) for i in range(inner)], -1)
    scale = reorder(down_scale[None], outer, inner, y)
    mixed = (summed * scale).astype(jnp.bfloat16)
    return reorder(mixed, outer, inner, (inner - y) % inner)


def hidden_chunks(width):
    whole = width // 128 * 128
    return [(0, whole - 256), (whole - 256, whole - 128), (whole, width), (whole - 128, whole)]


def columns(value, at, count):
    shift = at % 128
    if shift == 0:
        return value[:, at : at + count]
    low, high = at - shift, min(at - shift + count + 128, value.shape[1])
    return pltpu.roll(value[:, low:high], high - low - shift, 1)[:, :count]


def joined(gate, up, part, lo, hi):
    at = part * (gate.shape[1] // 2) + lo
    odd = (hi - lo) % 128
    even = hi - lo - odd
    pieces = [columns(gate, at, even), columns(up, at, even)] if even else []
    if odd:
        left = columns(gate, at + even, 128)
        right = pltpu.roll(columns(up, at + even, 128), odd, 1)
        lane = lax.broadcasted_iota(jnp.int32, left.shape, 1)
        pieces.append(jnp.where(lane < odd, left, right))
    return pieces


def units_of(outer, block):
    units = [(k // 2, k % 2, 0, block) for k in range(2 * outer - 1)]
    half = block // 2
    return units + [(outer - 1, 1, 0, half), (outer - 1, 1, half, half)]


def layer_kernel(outer, chunks, split, *refs):
    n = len(chunks)
    tokens, gain, gate, up, gate_scale, up_scale, down, down_scale, out = refs[:9]
    refs = refs[9:]
    raw_tok, raw_gate, raw_up, raw_down, scale = refs[:5]
    spare, allx, held, hid, part = refs[5 : n + 6], refs[n + 6], refs[n + 7 : 2 * n + 8], *refs[2 * n + 8 : 2 * n + 10]
    refs = refs[2 * n + 10 :]
    got_a, sum_a, sum_b, got_ba, got_bb, keep_a, keep_b, next_a, next_b, got_ca, got_cb, result, early_sum, head_sum = refs[:14]
    (
        raw_sem, w_recv, w_y, w_z, t_recv, t_send,
        a_send, a_recv, b_send, b_recv, c_send, c_recv,
    ) = refs[14:]
    items = n + 2
    x, me, c = lax.axis_index("rep"), lax.axis_index("fs"), lax.axis_index("tp")
    z, y = me // 2, lax.rem(me, 2)
    other = z * 2 + 1 - y
    rows, depth = raw_tok.shape
    height, block = spare[n].shape
    half = block // 2
    to_core, to_x, to_y = {"tp": 1 - c}, {"rep": 1 - x}, {"fs": other}
    up_ok, down_ok = z + 1 < outer, z > 0
    inside = down_ok & up_ok

    def at_z(step):
        return {"fs": me + 2 * step}

    span = pl.ds(pl.multiple_of(x * (2 * height), 128), 2 * height)
    low = height // 128 * 128
    own_part, other_part = (y * low, low + 128), ((1 - y) * (low + 128), low)

    def load_columns(source, target, part, at):
        lead, size = part
        return pltpu.make_async_copy(
            source.at[:, pl.ds(pl.multiple_of(x * (2 * height) + lead, 128), size)],
            target.at[:, pl.ds(pl.multiple_of(lead, 128), size)],
            raw_sem.at[at],
        )

    own_loads = [load_columns(gate, raw_gate, own_part, 0), load_columns(up, raw_up, own_part, 1)]
    other_loads = [
        load_columns(gate, raw_gate, other_part, 2), load_columns(up, raw_up, other_part, 3),
    ]
    late_loads = [
        pltpu.make_async_copy(tokens, raw_tok, raw_sem.at[4]),
        pltpu.make_async_copy(down.at[span], raw_down, raw_sem.at[5]),
    ]
    for load in (*own_loads, *other_loads, *late_loads):
        load.start()

    barrier = pltpu.get_barrier_semaphore()

    def greet(target):
        pl.semaphore_signal(
            barrier, inc=1, device_id=target, device_id_type=pl.DeviceIdType.MESH
        )

    for target in (to_core, to_x, to_y):
        greet(target)

    @pl.when(down_ok)
    def _():
        greet(at_z(-1))

    @pl.when(up_ok)
    def _():
        greet(at_z(1))

    def remote(source, target, send_sem, recv_sem, device):
        return pltpu.make_async_remote_copy(
            src_ref=source, dst_ref=target, send_sem=send_sem, recv_sem=recv_sem,
            device_id=device, device_id_type=pl.DeviceIdType.MESH,
        )

    def done(ref, sem):
        pltpu.make_async_copy(ref, ref, sem).wait()


    def slot(i, f):
        if i < n:
            return held[i].at[f]
        return held[n].at[f, pl.ds(0, height), pl.ds((i - n) * half, half)]

    def spare_of(i):
        return spare[i] if i < n else spare[n].at[:, pl.ds((i - n) * half, half)]

    def across_y(i):
        return remote(spare_of(i), slot(i, me), w_y.at[i], w_recv.at[i, me], to_y)

    def along(i, f, step):
        side = 0 if step < 0 else 1
        return remote(slot(i, f), slot(i, f), w_z.at[i, side], w_recv.at[i, f], at_z(step))

    def send_z(i, f, step):
        @pl.when(down_ok if step < 0 else up_ok)
        def _():
            along(i, f, step).start()

    def send_both(i, f):
        for step in (-1, 1):
            send_z(i, f, step)

    def take_other(i):
        done(slot(i, other), w_recv.at[i, other])

    def take(i, d, qs=(0, 1)):
        for sign in (1, -1):
            s = z + sign * d

            @pl.when((s < outer) if sign > 0 else (s >= 0))
            def _():
                for q in qs:
                    f = s * 2 + q
                    done(slot(i, f), w_recv.at[i, f])
                    send_z(i, f, -sign)

    def pack(i, sides=(0, 1)):
        for yy in range(2):

            @pl.when(y == yy)
            def _():
                for to, which in [((held[i].at[me], yy), (spare[i], 1 - yy))[side] for side in sides]:
                    at = 0
                    for piece in joined(raw_gate, raw_up, which, *chunks[i]):
                        to[:, at : at + piece.shape[1]] = piece.astype(to.dtype)
                        at += piece.shape[1]

    starts = [0]
    for lo, hi in chunks:
        starts.append(starts[-1] + 2 * (hi - lo))

    def pack_scale():
        tiles = 2 * height // 128
        gates, ups = (
            jnp.broadcast_to(
                jnp.concatenate([ref[pl.ds(x * tiles + i, 1)] for i in range(tiles)], 1),
                (8, 2 * height),
            )
            for ref in (gate_scale, up_scale)
        )
        for yy in range(2):

            @pl.when(y == yy)
            def _():
                at = 0
                for lo, hi in chunks:
                    for piece in joined(gates, ups, yy, lo, hi):
                        scale[:, at : at + piece.shape[1]] = piece
                        at += piece.shape[1]


    def place(cc, xx, yy):
        return cc * 4 + xx * 2 + yy

    mine, near_x, near_y, diagonal = (
        place(c, x, y), place(c, 1 - x, y), place(c, x, 1 - y), place(c, 1 - x, 1 - y)
    )
    half_rows = (rows - split) // 2
    spans = (pl.ds(0, split), pl.ds(split, half_rows), pl.ds(split + half_rows, half_rows))

    def move(t, h, device, at, seen_as):
        here = allx.at[t, spans[h]]
        return remote(here, here, t_send.at[at], t_recv.at[3 * seen_as + h], device)

    def moved(t, h, seen_as):
        done(allx.at[t, spans[h]], t_recv.at[3 * seen_as + h])

    def share(t, at):
        return remote(allx.at[t], allx.at[t], t_send.at[at], t_recv.at[at], to_core)

    own_x = [move(mine, h, to_x, h, 0) for h in range(3)]
    own_y = [move(mine, h, to_y, 3 + h, 1) for h in range(3)]
    relay_y = move(near_x, 0, to_y, 6, 2)
    relay_x = [move(near_y, 1 + i, to_x, 7 + i, 2) for i in range(2)]
    shares = [share(t, 9 + i) for i, t in enumerate((mine, near_x, near_y, diagonal))]

    def normalize():
        step = 64 if rows % 64 == 0 else 32

        def body(i, carry):
            at = pl.ds(pl.multiple_of(i * step, step), step)
            value = raw_tok[at].astype(jnp.float32)
            size = lax.rsqrt(jnp.mean(value * value, axis=-1, keepdims=True) + 1e-06)
            allx[mine, at] = (value * size * gain[...]).astype(allx.dtype)
            return carry

        lax.fori_loop(0, rows // step, body, 0)

    def early(i, d, qs=(0, 1)):
        @pl.when(inside)
        def _():
            take(i, d, qs)

    def late(i, ds, qs=(0, 1)):
        @pl.when(jnp.logical_not(inside))
        def _():
            for d in ds:
                take(i, d, qs)

    for load in own_loads:
        load.wait()
    pack(0, (0,))
    pl.semaphore_wait(
        barrier, 3 + jnp.minimum(z, 1) + jnp.minimum(outer - 1 - z, 1)
    )
    send_both(0, me)
    for load in other_loads:
        load.wait()
    pack(0, (1,))
    across_y(0).start()
    late_loads[0].wait()
    normalize()
    for h in range(3):
        own_x[h].start()
    own_y[1].start()
    pack(1)
    across_y(1).start()
    send_both(1, me)
    own_y[2].start()
    own_y[0].start()
    shares[0].start()
    for i in range(2, n):
        pack(i)
        across_y(i).start()
    late_loads[1].wait()
    for yy in range(2):

        @pl.when(y == yy)
        def _():
            spare[n][...] = raw_down[(1 - yy) * height : (2 - yy) * height].astype(spare[n].dtype)
            held[n][me, :height, :] = raw_down[yy * height : (yy + 1) * height].astype(held[n].dtype)

    for i in range(n, items):
        across_y(i).start()
    pack_scale()
    tail = held[n].shape[1] - height
    if tail:
        for f in range(2 * outer):
            held[n][f, height:, :] = jnp.zeros((tail, block), held[n].dtype)


    def silu(v):
        return v * (1.0 / (1.0 + jnp.exp(-v)))

    def store(t, both, lo, hi):
        odd = (hi - lo) % 128
        even = hi - lo - odd
        if even:
            value = silu(both[:, :even]) * both[:, even : 2 * even]
            hid[t, :, lo : lo + even] = value.astype(hid.dtype)
        if odd:
            both = both[:, 2 * even :]
            value = silu(both) * pltpu.roll(both, odd, 1)
            lane = lax.broadcasted_iota(jnp.int32, value.shape, 1)
            at = lo + even
            hid[t, :, at : at + 2 * odd] = jnp.where(lane < odd, value, 0.0).astype(hid.dtype)

    def scale_of(i):
        return scale[0:1, starts[i] : starts[i + 1]]

    def tile(k):
        j, cc = k // 2, c + (1 - 2 * c) * lax.rem(k, 2)
        return place(cc, x + (1 - 2 * x) * lax.rem(j, 2), y + (1 - 2 * y) * (j // 2))

    def hidden(i, start=0, stop=8):
        lo, hi = chunks[i]

        def body(k, carry):
            t = tile(k)
            both = jnp.dot(
                allx[t], held[i][...].reshape(depth, 2 * (hi - lo)),
                preferred_element_type=jnp.float32,
            )
            store(t, both * scale_of(i), lo, hi)
            return carry

        lax.fori_loop(start, stop, body, 0)


    deep = held[0].shape[1]
    near = jnp.where(z * 2 < outer, 0, 1)

    def reach(start, size):
        return pl.ds(pl.multiple_of(start, 2 * deep), size)

    def partly(i, t, start, planes_in):
        size = planes_in * 2 * deep
        return jnp.dot(
            allx[t, :, reach(start * 2 * deep, size)],
            held[i][pl.ds(start * 2, planes_in * 2)].reshape(size, held[i].shape[2]),
            preferred_element_type=jnp.float32,
        )

    def begin(i):
        lanes = starts[i + 1] - starts[i]

        def body(t, carry):
            early_sum[t, :, :lanes] = partly(i, t, near, outer - 1)
            return carry

        lax.fori_loop(0, 8, body, 0)

    def end(i, start=0, stop=8):
        lanes = starts[i + 1] - starts[i]

        def body(t, carry):
            both = early_sum[t, :, :lanes] + partly(i, t, (1 - near) * (outer - 1), 1)
            store(t, both * scale_of(i), *chunks[i])
            return carry

        lax.fori_loop(start, stop, body, 0)


    ready = chunks[1][1]

    def head():
        f = z * 2

        def body(t, carry):
            head_sum[t] = jnp.dot(
                hid[t, :, :ready], held[n][f, :ready], preferred_element_type=jnp.float32
            )
            return carry

        lax.fori_loop(0, 8, body, 0)

    last = n - 1
    distances = range(1, outer)
    moved(near_x, 0, 0)
    relay_y.start()
    take_other(0)
    send_both(0, other)
    early(0, 1)
    moved(near_y, 1, 1)
    relay_x[0].start()
    take_other(1)
    send_both(1, other)
    send_both(2, me)
    early(0, 2)
    moved(near_y, 2, 1)
    relay_x[1].start()
    early(1, 1)
    moved(near_x, 1, 0)
    moved(near_x, 2, 0)
    shares[1].start()
    take_other(2)
    send_both(2, other)
    moved(near_y, 0, 1)
    shares[2].start()
    early(1, 2)
    early(2, 1)
    for k in range(3):
        t = place(1 - c, *((x, y), (1 - x, y), (x, 1 - y))[k])
        done(allx.at[t], t_recv.at[9 + k])
    late(0, distances)
    hidden(0, 0, 6)
    for h in range(3):
        moved(diagonal, h, 2)
    shares[3].start()
    for i in range(n, items):
        take_other(i)
    early(2, 2)
    send_both(last, me)
    take_other(last)
    send_both(last, other)
    t = place(1 - c, 1 - x, 1 - y)
    done(allx.at[t], t_recv.at[12])
    hidden(0, 6, 8)
    early(last, 1)
    late(1, distances)
    hidden(1)
    early(last, 2)
    for q in range(2):
        for i in range(n, items):
            send_both(i, z * 2 + q)
    head()
    for i in range(2, n):
        late(i, range(1, outer - 1))
        begin(i)
        late(i, (outer - 1,))
        if i < last:
            end(i)


    planes = []
    for spot in range(outer):
        plane = 0
        for zz in range(outer):
            order = sorted(range(outer), key=lambda s: (abs(s - zz), -s))
            plane = plane + jnp.where(z == zz, order[spot], 0)
        planes.append(plane)
    units = units_of(outer, block)

    def high(k):
        return pl.ds(0, rows if units[k][3] == block else rows // 2)

    def send_a(k):
        wide_as = pl.ds(0, units[k][3])
        return remote(
            part.at[k % 2, pl.ds((1 - c) * 4, 4), :, wide_as], got_a.at[k, :, :, wide_as],
            a_send.at[k % 2], a_recv.at[k], to_core,
        )

    def send_b(k):
        return [
            remote(
                sums.at[k % 3, pl.ds((1 - first) * 2, 2), high(k)], got.at[k, :, high(k)],
                b_send.at[k % 3, i], b_recv.at[k, i], to,
            )
            for i, (sums, first, got, to) in enumerate(
                ((sum_a, x, got_ba, to_x), (sum_b, y, got_bb, to_y))
            )
        ]

    def send_c(k):
        return [
            remote(
                source.at[k % 3, high(k)], got.at[k, high(k)], c_send.at[k % 3, i], c_recv.at[k, i], to
            )
            for i, (source, got, to) in enumerate(((next_a, got_ca, to_y), (next_b, got_cb, to_x)))
        ]

    def wide(value):
        return value.astype(jnp.float32)

    def multiply(k):
        if k >= 2:
            send_a(k - 2).wait_send()
        spot, q, lo, count = units[k]
        f = planes[spot] * 2 + q

        def body(t, carry):
            if k:
                total = jnp.dot(
                    hid[t], held[n][f, :, lo : lo + count], preferred_element_type=jnp.float32
                )
            else:
                total = head_sum[t] + jnp.dot(
                    hid[t, :, ready:], held[n][f, ready:], preferred_element_type=jnp.float32
                )
            part[k % 2, t, :, 0:count] = total.astype(part.dtype)
            return carry

        for turn, at in enumerate(((1 - c) * 4, c * 4)):
            if k == 0:
                end(last, at, at + 4)
            lax.fori_loop(at, at + 4, body, 0)
            if turn == 0:
                send_a(k).start()

    def first(k):
        count = units[k][3]
        done(got_a.at[k, :, :, pl.ds(0, count)], a_recv.at[k])
        if k >= 3:
            for copy in send_b(k - 3):
                copy.wait_send()

        def body(i, carry):
            total = wide(part[k % 2, c * 4 + i, :, 0:count]) + wide(got_a[k, i, :, 0:count])
            total = total.astype(part.dtype)
            turned = lax.rem(i, 2) * 2 + i // 2
            if count == block:
                sum_a[k % 3, i] = total[:, :half]
                sum_b[k % 3, turned] = total[:, half:]
            else:
                sum_a[k % 3, i, : rows // 2] = total[: rows // 2]
                sum_b[k % 3, turned, : rows // 2] = total[rows // 2 :]
            return carry

        lax.fori_loop(0, 4, body, 0)
        for copy in send_b(k):
            copy.start()

    def second(k):
        h, s = high(k), k % 3
        for i, got in enumerate((got_ba, got_bb)):
            done(got.at[k, :, h], b_recv.at[k, i])
        if k >= 3:
            for copy in send_c(k - 3):
                copy.wait_send()
        next_a[s, h] = (wide(sum_a[s, x * 2 + 1 - y, h]) + wide(got_ba[k, 1 - y, h])).astype(next_a.dtype)
        next_b[s, h] = (wide(sum_b[s, y * 2 + 1 - x, h]) + wide(got_bb[k, 1 - x, h])).astype(next_b.dtype)
        for copy in send_c(k):
            copy.start()
        keep_a[s, h] = wide(sum_a[s, x * 2 + y, h]) + wide(got_ba[k, y, h])
        keep_b[s, h] = wide(sum_b[s, y * 2 + x, h]) + wide(got_bb[k, x, h])

    def third(k):
        h, s = high(k), k % 3
        for i, got in enumerate((got_ca, got_cb)):
            done(got.at[k, h], c_recv.at[k, i])
        spot, q, lo, count = units[k]
        base = (planes[spot] * 2 + q) * block
        for i, (keep, got) in enumerate(((keep_a, got_ca), (keep_b, got_cb))):
            if count == block:
                lead, down_rows = i * half, pl.ds(0, rows)
            else:
                lead, down_rows = lo, pl.ds(i * (rows // 2), rows // 2)
            at = pl.ds(pl.multiple_of(base + lead, half), half)
            result[down_rows, at] = ((keep[s, h] + wide(got[k, h])) * down_scale[:, at]).astype(out.dtype)

    def write(k):
        spot, q, lo, count = units[k]
        at = pl.ds(pl.multiple_of((planes[spot] * 2 + q) * block + lo, half), count)
        return pltpu.make_async_copy(result.at[:, at], out.at[:, at], raw_sem.at[k])

    def finish(k):
        third(k)
        write(k).start()

    count = len(units)
    for k in range(count):
        if 1 <= k <= 4:
            for i in range(n, items):
                early(i, (k + 1) // 2, ((k - 1) % 2,))
        spot, q, lo, size = units[k]
        if spot >= 1:
            for i in range(n, items):
                if size == block or (i - n) * half == lo:
                    late(i, (spot,), (q,))
        multiply(k)
        first(k)
        if 1 <= k < count - 2:
            second(k - 1)
        if 3 <= k < count - 1:
            finish(k - 3)
    second(count - 3)
    second(count - 2)
    finish(count - 4)
    second(count - 1)
    def sent(i, planes_sent, side):
        many = pl.ds(0, 2 * planes_sent)
        if i < n:
            done(held[i].at[many], w_z.at[i, side])
        else:
            lanes = pl.ds((i - n) * half, half)
            done(held[n].at[many, pl.ds(0, height), lanes], w_z.at[i, side])

    for i in range(items):
        across_y(i).wait_send()
    for zz in range(outer):

        @pl.when(z == zz)
        def _():
            for i in range(items):
                if zz > 0:
                    sent(i, outer - zz, 0)
                if zz + 1 < outer:
                    sent(i, zz + 1, 1)

    for copy in (*own_x, *own_y, relay_y, *relay_x, *shares):
        copy.wait_send()
    for k in range(count - 3, count):
        finish(k)
    for k in range(count):
        write(k).wait()
    for k in range(count - 3, count):
        for copy in (*send_b(k), *send_c(k)):
            copy.wait_send()
    for k in range(count - 2, count):
        send_a(k).wait_send()


def fused_layer(outer, tokens, gain, gate, up, gate_scale, up_scale, down, down_scale):
    rows, depth = tokens.shape
    deep, width = gate.shape
    height, block, count = width // 4, down.shape[1], 2 * outer
    half = block // 2
    padded = -(-height // 128) * 128
    chunks = hidden_chunks(height)
    n = len(chunks)
    kind = jnp.bfloat16

    def room(*shape, dtype=kind):
        return pltpu.VMEM(shape, dtype)

    anywhere = pl.BlockSpec(memory_space=pl.ANY)
    inside = pl.BlockSpec(memory_space=pltpu.VMEM)
    dma = pltpu.SemaphoreType.DMA
    units = len(units_of(outer, block))
    return pl.pallas_call(
        functools.partial(layer_kernel, outer, chunks, rows // 96 * 16),
        out_shape=jax.ShapeDtypeStruct((rows, depth), kind),
        in_specs=[anywhere, inside, anywhere, anywhere, inside, inside, anywhere, inside],
        out_specs=anywhere,
        scratch_shapes=[
            room(rows, depth),
            room(deep, 2 * height, dtype=jnp.float32),
            room(deep, 2 * height, dtype=jnp.float32),
            room(2 * height, block, dtype=jnp.float32),
            room(8, 2 * height, dtype=jnp.float32),
            *(room(deep, 2 * (hi - lo)) for lo, hi in chunks),
            room(height, block),
            room(8, rows, depth),
            *(room(count, deep, 2 * (hi - lo)) for lo, hi in chunks),
            room(count, padded, block),
            room(8, rows, padded),
            room(2, 8, rows, block),
            room(units, 4, rows, block),
            room(3, 4, rows, half),
            room(3, 4, rows, half),
            room(units, 2, rows, half),
            room(units, 2, rows, half),
            room(3, rows, half, dtype=jnp.float32),
            room(3, rows, half, dtype=jnp.float32),
            room(3, rows, half),
            room(3, rows, half),
            room(units, rows, half),
            room(units, rows, half),
            room(rows, depth),
            room(8, rows, 256, dtype=jnp.float32),
            room(8, rows, block, dtype=jnp.float32),
            dma((max(units, 6),)),
            dma((n + 2, count)),
            dma((n + 2,)),
            dma((n + 2, 2)),
            dma((13,)),
            dma((13,)),
            dma((2,)),
            dma((units,)),
            dma((3, 2)),
            dma((units, 2)),
            dma((3, 2)),
            dma((units, 2)),
        ],
        compiler_params=pltpu.CompilerParams(
            collective_id=1, has_side_effects=True, vmem_limit_bytes=67043328
        ),
        cost_estimate=pl.CostEstimate(
            flops=48 * rows * depth * height, bytes_accessed=8 * rows * depth, transcendentals=0
        ),
    )(tokens, gain, gate, up, gate_scale, up_scale, down, down_scale)


def on_plane(
    tokens, norm_gain, gate_weight, up_weight, gate_scale, up_scale, down_weight, down_scale
):
    outer, _ = grid_of(lax.axis_size("fs"))
    return fused_layer(
        outer, tokens, norm_gain[None], gate_weight, up_weight,
        gate_scale.reshape(-1, 128), up_scale.reshape(-1, 128), down_weight, down_scale[None],
    )


def planar(mesh, tokens, gate_weight):
    sizes = mesh.shape
    if grid_of(sizes["fs"]) != (4, 2) or sizes["rep"] != 2 or sizes["tp"] != 2:
        return False
    width, rows = gate_weight.shape[1] // 8, tokens.shape[0] // mesh.size
    depth = gate_weight.shape[0]
    return (
        gate_weight.shape[1] % 8 == 0 and width % 128 == 64 and width > 256
        and rows % 96 == 0 and depth % (sizes["fs"] * 256) == 0
    )


def solution(mesh):
    placed = (
        P(("rep", "fs", "tp"), None),
        P(),
        P("fs", "tp"),
        P("fs", "tp"),
        P("tp"),
        P("tp"),
        P("tp", "fs"),
        P(),
    )

    def layer(tokens, norm_gain, gate_weight, *rest):
        return jax.shard_map(
            on_plane if planar(mesh, tokens, gate_weight) else on_device,
            mesh=mesh,
            in_specs=placed,
            out_specs=P(("rep", "fs", "tp"), None),
            check_vma=False,
        )(tokens, norm_gain, gate_weight, *rest)

    return layer
```
